128 devices in a mesh: ep: 16 (over z, x), tp: 8 (over y, core).
Axes of the slice: x: 4, y: 4, z: 4, core: 2. Of those that a mesh axis runs over, the one named last changes fastest.
Arguments:
- hidden_in: bfloat16 [256, 2048], P(None, 'ep'), may hold values from -24 to 24
- attn_gain: float32 [2048], replicated, may hold values from 0.1 to 1.9
- forget_weight: bfloat16 [2048, 16], replicated, may hold values from -0.125 to 0.125
- forget_bias: float32 [16], replicated, may hold values from -1 to 2
- query_weight: bfloat16 [2048, 2048], P('ep', 'tp'), may hold values from -0.125 to 0.125
- key_weight: bfloat16 [2048, 1024], P('ep', 'tp'), may hold values from -0.125 to 0.125
- value_weight: bfloat16 [2048, 1024], P('ep', 'tp'), may hold values from -0.125 to 0.125
- query_gain: float32 [128], replicated, may hold values from 0.1 to 1.9
- key_gain: float32 [128], replicated, may hold values from 0.1 to 1.9
- cache_keys: bfloat16 [256, 8, 1024, 128], P('ep', 'tp'), may hold values from -160 to 160
- cache_values: bfloat16 [256, 8, 1024, 128], P('ep', 'tp'), may hold values from -6 to 6
- cache_gates: float32 [256, 16, 1024], P('ep', 'tp'), may hold values from -256 to 0, as said below
- lengths: int32 [256], P('ep'), may hold values from 128 to 1024, as said below
- output_weight: bfloat16 [2048, 2048], P('tp', 'ep'), may hold values from -0.125 to 0.125
- ffn_gain: float32 [2048], replicated, may hold values from 0.1 to 1.9
- route_group: int32 [256], replicated, may hold values from 0 to 7, as said below
- route_expert: int32 [256, 2], replicated, may hold values from 0 to 3, as said below
- route_weight: float32 [256, 2], replicated, may hold values from 0.1 to 0.6
- expert_gate: bfloat16 [32, 2048, 1024], P('ep', None, 'tp'), may hold values from -0.125 to 0.125
- expert_up: bfloat16 [32, 2048, 1024], P('ep', None, 'tp'), may hold values from -0.125 to 0.125
- expert_down: bfloat16 [32, 1024, 2048], P('ep', 'tp'), may hold values from -0.1875 to 0.1875
- mix_vector: bfloat16 [2048], replicated, may hold values from -0.125 to 0.125
- dense_gate: bfloat16 [2048, 4096], P('ep', 'tp'), may hold values from -0.125 to 0.125
- dense_up: bfloat16 [2048, 4096], P('ep', 'tp'), may hold values from -0.125 to 0.125
- dense_down: bfloat16 [4096, 2048], P('tp', 'ep'), may hold values from -0.09375 to 0.09375
Outputs:
- mixed: bfloat16 [256, 2048], P(None, 'ep')
- fresh_keys: bfloat16 [256, 1024], P('ep', 'tp')
- fresh_values: bfloat16 [256, 1024], P('ep', 'tp')
The draws below stay inside these ranges and needn't reach their ends.
Inputs may be any that keep to these rules, and one draw needn't show every extreme that they name: `cache_gates`: never rising along positions. `lengths`: some device holds a sequence of length 1024 in every draw. `route_group`: no expert is chosen by more than 24 tokens of the batch, and some expert by exactly 24. `route_expert`: a token's 2 experts differ; the loads of the experts of one group differ by at most two.
All inputs are finite; a program needn't handle non-finite values.
Results may differ from the reference program's by a relative error of at most 0.008.
Values may be sent and summed in bfloat16 or wider, within the bound.
A program may use at most 64 MiB of HBM per device.

```python
import jax
import jax.numpy as jnp
from jax import lax

D = 2048
QUERY_HEADS = 16
KV_HEADS = 8
HEAD_DIM = 128
EXPERT_WIDTH = 1024
DENSE_WIDTH = 4096
GROUP_EXPERTS = 4
TOPK = 2
SEQ_DEV = 16
CACHE_POSITIONS = 1024
SEQUENCE_COUNT = 256
EXPERTS = 32
GROUPS = 8
CAPACITY = 24


def draw_hidden_in(key, part):
    key_col, key_val = jax.random.split(key, 2)
    position = jnp.arange(D, dtype=jnp.float32) / D
    noise_level = jax.random.uniform(key_col, (D,), jnp.float32, 0.6, 1.4)
    column_scale = 3.0 ** position * noise_level * 0.6
    values = jax.random.normal(key_val, (SEQUENCE_COUNT, D), jnp.float32) * column_scale
    return jnp.clip(values, -24.0, 24.0).astype(jnp.bfloat16)


def draw_cache_keys(key, part):
    key_val = jax.random.fold_in(key, 0)
    values = jax.random.normal(key_val, (SEQUENCE_COUNT, KV_HEADS, CACHE_POSITIONS, HEAD_DIM), jnp.float32)
    return jnp.clip(values, -160.0, 160.0).astype(jnp.bfloat16)


def draw_cache_gates(key, part):
    kind_random_key, fast_random_key, slow_random_key, rough_random_key, spike_random_key, depth_random_key = jax.random.split(key, 6)
    chooser = jax.random.uniform(kind_random_key, (SEQUENCE_COUNT, QUERY_HEADS, 1), jnp.float32)
    fast_flag = chooser < 0.5
    fast_rate = 1.0 / jax.random.uniform(fast_random_key, (SEQUENCE_COUNT, QUERY_HEADS, 1), jnp.float32, 10.0, 40.0)
    slow_rate = jax.random.uniform(slow_random_key, (SEQUENCE_COUNT, QUERY_HEADS, 1), jnp.float32, 0.3, 1.5) / CACHE_POSITIONS
    drift_rate = jnp.where(fast_flag, fast_rate, slow_rate)
    noise_level = jax.random.uniform(rough_random_key, (SEQUENCE_COUNT, QUERY_HEADS, CACHE_POSITIONS), jnp.float32, 0.3, 1.7)
    spike_position = jax.random.uniform(spike_random_key, (SEQUENCE_COUNT, QUERY_HEADS, CACHE_POSITIONS), jnp.float32) < 3.0 / CACHE_POSITIONS
    spike_depth = jnp.log(jax.random.uniform(depth_random_key, (SEQUENCE_COUNT, QUERY_HEADS, CACHE_POSITIONS), jnp.float32, 0.5, 0.8))
    step_increments = -drift_rate * noise_level + jnp.where(spike_position & jnp.logical_not(fast_flag), spike_depth, 0.0)
    return jnp.cumsum(step_increments, axis=2).astype(jnp.float32)


def draw_lengths(key, part):
    key_len, key_pick = jax.random.split(key)
    drawn = jax.random.randint(key_len, (SEQUENCE_COUNT,), CACHE_POSITIONS // 8, CACHE_POSITIONS + 1)
    block_count = SEQUENCE_COUNT // SEQ_DEV
    picked = jax.random.randint(key_pick, (block_count, 1), 0, SEQ_DEV)
    full_length = jnp.arange(SEQ_DEV, dtype=jnp.int32)[None, :] == picked
    return jnp.where(full_length.reshape(SEQUENCE_COUNT), CACHE_POSITIONS, drawn).astype(jnp.int32)


def route_tables(key):
    folded = jax.random.fold_in(key, 11)
    key_size, key_label, key_token, key_expert = jax.random.split(folded, 4)
    mean_size = SEQUENCE_COUNT // GROUPS
    half_size = mean_size // 2
    swings = jax.random.randint(key_size, ((GROUPS - 2) // 2,), 0, half_size + 1)
    group_sizes = jnp.concatenate([jnp.array([mean_size + half_size, mean_size - half_size], jnp.int32), mean_size + swings, mean_size - swings]).astype(jnp.int32)
    group_sizes = group_sizes[jax.random.permutation(key_label, GROUPS)]
    group_ends = jnp.cumsum(group_sizes)
    starts = group_ends - group_sizes
    token_rank = jax.random.permutation(key_token, SEQUENCE_COUNT).astype(jnp.int32)
    group_of = jnp.sum((token_rank[:, None] >= group_ends[None, :]).astype(jnp.int32), axis=1)
    position = token_rank - starts[group_of]
    first_pick = position % GROUP_EXPERTS
    second = (first_pick + 1 + position // GROUP_EXPERTS % (GROUP_EXPERTS - 1)) % GROUP_EXPERTS
    labels = jax.vmap(lambda subkey: jax.random.permutation(subkey, GROUP_EXPERTS))(jax.random.split(key_expert, GROUPS)).astype(jnp.int32)
    both_picks = jnp.stack([first_pick, second], axis=1)
    experts = jnp.take_along_axis(labels[group_of], both_picks, axis=1)
    return (group_of.astype(jnp.int32), experts.astype(jnp.int32))


def draw_route_group(key, part):
    return route_tables(key)[0]


def draw_route_expert(key, part):
    return route_tables(key)[1]


def levels(key, shape, cuts, low, high):
    factor_of = 1.0
    for dim, shards_of in cuts:
        steps = jax.random.uniform(jax.random.fold_in(jax.random.fold_in(key, 6), dim), (shards_of,), jnp.float32, low / len(cuts), high / len(cuts))
        factor_of = factor_of * jnp.repeat(jnp.exp(steps), shape[dim] // shards_of).reshape((-1,) + (1,) * (len(shape) - 1 - dim))
    return factor_of


def gaussian(stream_key, extent, scale, most, cuts=(), kind=jnp.bfloat16):
    values = jax.random.normal(stream_key, extent, jnp.float32) * scale
    if len(cuts) > 0:
        values = levels(stream_key, extent, cuts, -0.22, 0.18) * values
    return jnp.clip(values, min=-most, max=most).astype(kind)


def setup_inputs(seed: int = 0) -> dict:
    seeds = jax.random.split(jax.random.key(seed), 26)
    hidden_in = draw_hidden_in(jax.random.fold_in(seeds[25], 71), 0)
    attn_gain = jnp.clip(1.0 + 0.18 * jax.random.normal(seeds[1], (D,), jnp.float32), 0.1, 1.9)
    forget_weight = gaussian(seeds[2], (D, QUERY_HEADS), D ** -0.5, 0.125)
    forget_bias = jnp.clip(jax.random.uniform(seeds[3], (QUERY_HEADS,), jnp.float32, -1.0, 2.0), -1.0, 2.0)
    query_weight = gaussian(seeds[4], (D, QUERY_HEADS * HEAD_DIM), D ** -0.5, 0.125, ((0, 16), (1, 8)))
    key_weight = gaussian(seeds[5], (D, KV_HEADS * HEAD_DIM), D ** -0.5, 0.125, ((0, 16), (1, 8)))
    value_weight = gaussian(seeds[6], (D, KV_HEADS * HEAD_DIM), D ** -0.5, 0.125, ((0, 16), (1, 8)))
    query_gain = jnp.clip(1.0 + 0.18 * jax.random.normal(seeds[7], (HEAD_DIM,), jnp.float32), 0.1, 1.9)
    key_gain = jnp.clip(1.0 + 0.18 * jax.random.normal(seeds[8], (HEAD_DIM,), jnp.float32), 0.1, 1.9)
    cache_keys = draw_cache_keys(jax.random.fold_in(seeds[25], 71), 0)
    cache_values = gaussian(seeds[10], (SEQUENCE_COUNT, KV_HEADS, CACHE_POSITIONS, HEAD_DIM), 1.0, 6.0, ((0, 16), (1, 8)))
    cache_gates = draw_cache_gates(jax.random.fold_in(seeds[25], 71), 0)
    lengths = draw_lengths(jax.random.fold_in(seeds[25], 71), 0)
    output_weight = gaussian(seeds[13], (QUERY_HEADS * HEAD_DIM, D), (QUERY_HEADS * HEAD_DIM) ** -0.5, 0.125, ((0, 8), (1, 16)))
    ffn_gain = jnp.clip(1.0 + 0.18 * jax.random.normal(seeds[14], (D,), jnp.float32), 0.1, 1.9)
    route_group = draw_route_group(jax.random.fold_in(seeds[25], 71), 0)
    route_expert = draw_route_expert(jax.random.fold_in(seeds[25], 71), 0)
    route_weight = jnp.clip(jax.random.uniform(seeds[17], (SEQUENCE_COUNT, TOPK), jnp.float32, 0.1, 0.6), 0.1, 0.6)
    expert_gate = gaussian(seeds[18], (EXPERTS, D, EXPERT_WIDTH), D ** -0.5, 0.125, ((0, 16), (2, 8)))
    expert_up = gaussian(seeds[19], (EXPERTS, D, EXPERT_WIDTH), D ** -0.5, 0.125, ((0, 16), (2, 8)))
    expert_down = gaussian(seeds[20], (EXPERTS, EXPERT_WIDTH, D), EXPERT_WIDTH ** -0.5, 0.1875, ((0, 16), (1, 8)))
    mix_vector = gaussian(seeds[21], (D,), D ** -0.5, 0.125)
    dense_gate = gaussian(seeds[22], (D, DENSE_WIDTH), D ** -0.5, 0.125, ((0, 16), (1, 8)))
    dense_up = gaussian(seeds[23], (D, DENSE_WIDTH), D ** -0.5, 0.125, ((0, 16), (1, 8)))
    dense_down = gaussian(seeds[24], (DENSE_WIDTH, D), DENSE_WIDTH ** -0.5, 0.09375, ((0, 8), (1, 16)))
    return dict(hidden_in=hidden_in, attn_gain=attn_gain, forget_weight=forget_weight, forget_bias=forget_bias, query_weight=query_weight, key_weight=key_weight, value_weight=value_weight, query_gain=query_gain, key_gain=key_gain, cache_keys=cache_keys, cache_values=cache_values, cache_gates=cache_gates, lengths=lengths, output_weight=output_weight, ffn_gain=ffn_gain, route_group=route_group, route_expert=route_expert, route_weight=route_weight, expert_gate=expert_gate, expert_up=expert_up, expert_down=expert_down, mix_vector=mix_vector, dense_gate=dense_gate, dense_up=dense_up, dense_down=dense_down)


EPS = 1e-06

def head_norm(projected, gain_vec):
    return projected * lax.rsqrt(lax.optimization_barrier(jnp.mean(projected * projected, axis=-1, keepdims=True)) + EPS) * gain_vec

def slot_targets(route_group, route_expert):
    chosen = (route_group[:, None] * GROUP_EXPERTS + route_expert).reshape(-1).astype(jnp.int32)
    onehot = (chosen[:, None] == jnp.arange(EXPERTS, dtype=jnp.int32)[None, :]).astype(jnp.int32)
    before = jnp.cumsum(onehot, axis=0) - onehot
    return (chosen * CAPACITY + lax.optimization_barrier(jnp.sum(before * onehot, axis=1))).astype(jnp.int32)

def reference(hidden_in, attn_gain, forget_weight, forget_bias, query_weight, key_weight, value_weight, query_gain, key_gain, cache_keys, cache_values, cache_gates, lengths, output_weight, ffn_gain, route_group, route_expert, route_weight, expert_gate, expert_up, expert_down, mix_vector, dense_gate, dense_up, dense_down):
    stream = hidden_in.astype(jnp.float32)
    normed_in = (stream * attn_gain).astype(jnp.bfloat16)
    inv_rms = lax.rsqrt(lax.optimization_barrier(jnp.mean(stream * stream, axis=1)) + EPS)
    query_rows = head_norm(jnp.dot(normed_in, query_weight, preferred_element_type=jnp.float32).reshape(SEQUENCE_COUNT, QUERY_HEADS, HEAD_DIM), query_gain).astype(jnp.bfloat16)
    fresh_keys = head_norm(jnp.dot(normed_in, key_weight, preferred_element_type=jnp.float32).reshape(SEQUENCE_COUNT, KV_HEADS, HEAD_DIM), key_gain).astype(jnp.bfloat16)
    fresh_values = (jnp.dot(normed_in, value_weight, preferred_element_type=jnp.float32) * inv_rms[:, None]).astype(jnp.bfloat16)
    log_forget = jax.nn.log_sigmoid(jnp.dot(normed_in, forget_weight, preferred_element_type=jnp.float32) * inv_rms[:, None] + forget_bias)
    latest = jnp.take_along_axis(cache_gates, (lengths - 1).astype(jnp.int32)[:, None, None], axis=2)[:, :, 0]
    now_gate = latest + log_forget
    group_size = QUERY_HEADS // KV_HEADS
    factor = HEAD_DIM ** (-0.5)
    positions = jnp.arange(CACHE_POSITIONS, dtype=jnp.int32)

    def one_sequence(items):
        query_one, keys_one, values_one, gates_one, now_one, length_one, key_new, value_new = items
        grouped = query_one.astype(jnp.float32).reshape(KV_HEADS, group_size, HEAD_DIM)
        scores = jnp.einsum('kgd,kcd->kgc', grouped, keys_one.astype(jnp.float32)) * factor
        scores = scores + now_one.reshape(KV_HEADS, group_size, 1) - gates_one.reshape(KV_HEADS, group_size, CACHE_POSITIONS)
        scores = jnp.where(positions < length_one, scores, -jnp.inf)
        new_key = key_new.astype(jnp.float32).reshape(KV_HEADS, 1, HEAD_DIM)
        self_score = lax.optimization_barrier(jnp.sum(grouped * new_key, axis=-1)) * factor
        ceiling = jnp.maximum(lax.optimization_barrier(jnp.max(scores, axis=-1)), self_score)
        weights = jnp.exp(scores - ceiling[:, :, None])
        self_weight = jnp.exp(self_score - ceiling)
        denominator = lax.optimization_barrier(jnp.sum(weights, axis=-1)) + self_weight
        rounded = lax.optimization_barrier(weights.astype(jnp.bfloat16)).astype(jnp.float32)
        summed = jnp.einsum('kgc,kcd->kgd', rounded, values_one.astype(jnp.float32))
        summed = summed + self_weight[:, :, None] * value_new.astype(jnp.float32).reshape(KV_HEADS, 1, HEAD_DIM)
        return (summed / denominator[:, :, None]).reshape(QUERY_HEADS * HEAD_DIM).astype(jnp.bfloat16)
    heads_out = lax.map(one_sequence, (query_rows, cache_keys, cache_values, cache_gates, now_gate, lengths, fresh_keys, fresh_values.reshape(SEQUENCE_COUNT, KV_HEADS, HEAD_DIM)))
    middle = (stream + jnp.dot(heads_out, output_weight, preferred_element_type=jnp.float32)).astype(jnp.bfloat16)
    middle_f = middle.astype(jnp.float32)
    normed_mid = (middle_f * ffn_gain).astype(jnp.bfloat16)
    mid_scale = lax.rsqrt(lax.optimization_barrier(jnp.mean(middle_f * middle_f, axis=1)) + EPS)
    mix_share = jax.nn.sigmoid(mid_scale * jnp.dot(normed_mid, mix_vector, preferred_element_type=jnp.float32))
    targets = slot_targets(route_group, route_expert)
    token_ids = jnp.arange(SEQUENCE_COUNT * TOPK, dtype=jnp.int32) // TOPK
    slot_rows = jnp.zeros((EXPERTS * CAPACITY, D), jnp.bfloat16).at[targets].set(normed_mid[token_ids])
    slot_scale = jnp.zeros((EXPERTS * CAPACITY,), jnp.float32).at[targets].set(mid_scale[token_ids])

    def one_expert(items):
        block_rows, block_scale, gate_matrix, up_matrix, down_matrix = items
        gate_pre = jnp.dot(block_rows, gate_matrix, preferred_element_type=jnp.float32) * block_scale[:, None]
        up_pre = jnp.dot(block_rows, up_matrix, preferred_element_type=jnp.float32) * block_scale[:, None]
        hidden_units = (jax.nn.silu(gate_pre) * up_pre).astype(jnp.bfloat16)
        return jnp.dot(hidden_units, down_matrix, preferred_element_type=jnp.float32)
    expert_out = lax.map(one_expert, (slot_rows.reshape(EXPERTS, CAPACITY, D), slot_scale.reshape(EXPERTS, CAPACITY), expert_gate, expert_up, expert_down)).reshape(EXPERTS * CAPACITY, D)
    picked = expert_out[targets].reshape(SEQUENCE_COUNT, TOPK, D)
    routed = lax.optimization_barrier(jnp.sum(picked * route_weight[:, :, None], axis=1))
    dense_gate_pre = jnp.dot(normed_mid, dense_gate, preferred_element_type=jnp.float32) * mid_scale[:, None]
    dense_up_pre = jnp.dot(normed_mid, dense_up, preferred_element_type=jnp.float32) * mid_scale[:, None]
    dense_hidden = (jax.nn.silu(dense_gate_pre) * dense_up_pre).astype(jnp.bfloat16)
    dense_result = jnp.dot(dense_hidden, dense_down, preferred_element_type=jnp.float32)
    mixed = (middle_f + routed + mix_share[:, None] * dense_result).astype(jnp.bfloat16)
    return (mixed, fresh_keys.reshape(SEQUENCE_COUNT, KV_HEADS * HEAD_DIM), fresh_values)
```

```python
import jax
import jax.numpy as jnp
from jax import lax
from jax.experimental import pallas as pl
from jax.experimental.pallas import tpu as pltpu
from jax.sharding import PartitionSpec as P

D = 2048
HEAD = 128
GROUP_EXPERTS = 4
CAPACITY = 24
EXPERTS = 32
SEQS = 256
EP = 16
TP = 8
OWN = SEQS // EP
EPS = 1e-06
FACTOR = HEAD**-0.5
F32 = jnp.float32
BF16 = jnp.bfloat16
MESH_ID = pl.DeviceIdType.MESH
NT = (((1,), (1,)), ((), ()))

EP_OFFSETS = sorted(
    [(dz, dx) for dz in range(4) for dx in range(4) if (dz, dx) != (0, 0)],
    key=lambda o: -(min(o[0], 4 - o[0]) + min(o[1], 4 - o[1])),
)
TP_OFFSETS = [4, 5, 3, 2, 6, 7, 1]


def mm(a, b):
    return jnp.dot(a, b, preferred_element_type=F32)


def iota(shape, dim):
    return lax.broadcasted_iota(jnp.int32, shape, dim)


def silu(v):
    return v * jax.nn.sigmoid(v)


def layer(
    hidden, attn_gain, forget_t, forget_bias, query_w, key_w, value_w, query_gain, key_gain,
    cache_k, cache_v, cache_g, lengths, output_w, ffn_gain, group, expert_t, weight_t,
    gate_w, up_w, down_w, mix_vector, dense_gate, dense_up, dense_down,
    mixed_out, keys_out, values_out,
    hid, again, fwt, fbias, wqkv, qgain, kgain, kcat, vbuf, graw, lens, wout, fgain,
    grp, ext, wtt, wgu, wdn, mixv, wdense, wdd,
    send1, recv1, gates, place, place_t, heads, part, psend, precv, mid,
    send4, xrows, send4d, recv4d, send5, ret, dhid, part2, psend2, precv2, final,
    load_sem, kv_sem, ep_send, ep_recv, tp_send, tp_recv, out_sem,
):
    e = lax.axis_index("ep")
    t = lax.axis_index("tp")
    z = lax.div(e, 4)
    x = lax.rem(e, 4)
    ep_peers = [
        (dz * 4 + dx, lax.rem(z + dz, 4) * 4 + lax.rem(x + dx, 4)) for dz, dx in EP_OFFSETS
    ]
    tp_peers = [(j, lax.rem(t + j, TP)) for j in TP_OFFSETS]
    own_cols = pl.ds(pl.multiple_of(e * HEAD, HEAD), HEAD)

    barrier = pltpu.get_barrier_semaphore()
    for _, peer in ep_peers:
        pl.semaphore_signal(barrier, inc=1, device_id={"ep": peer}, device_id_type=MESH_ID)
    for _, peer in tp_peers:
        pl.semaphore_signal(barrier, inc=1, device_id={"tp": peer}, device_id_type=MESH_ID)

    loads = {}

    def load(name, src, dst):
        copy = pltpu.make_async_copy(src, dst, load_sem.at[len(loads)])
        copy.start()
        loads[name] = copy

    load("hid", hidden, hid)
    load("again", attn_gain, again)
    load("fwt", forget_t.at[:, own_cols], fwt.at[pl.ds(0, 16)])
    load("wq", query_w, wqkv.at[:, pl.ds(0, 256)])
    load("wk", key_w, wqkv.at[:, pl.ds(256, 128)])
    load("wv", value_w, wqkv.at[:, pl.ds(384, 128)])
    load("grp", group, grp)
    load("ext", expert_t, ext)
    load("wtt", weight_t, wtt)
    load("graw", cache_g, graw)
    load("lens", lengths, lens)
    load("fbias", forget_bias, fbias)
    load("qgain", query_gain, qgain)
    load("kgain", key_gain, kgain)
    kv = []
    for b in range(OWN):
        copy = pltpu.make_async_copy(
            cache_k.at[b], kcat.at[:, pl.ds(b * HEAD, HEAD)], kv_sem.at[0, b]
        )
        copy.start()
        kv.append(copy)
    for b in range(OWN):
        copy = pltpu.make_async_copy(cache_v.at[b], vbuf.at[b], kv_sem.at[1, b])
        copy.start()
        kv.append(copy)
    load("wout", output_w, wout)
    load("fgain", ffn_gain, fgain)
    load("mixv", mix_vector, mixv)
    load("dg", dense_gate, wdense.at[:, pl.ds(0, 512)])
    load("du", dense_up, wdense.at[:, pl.ds(512, 512)])
    load("dd", dense_down, wdd)
    for i in range(2):
        load(f"g{i}", gate_w.at[i], wgu.at[:, pl.ds(i * 128, 128)])
        load(f"u{i}", up_w.at[i], wgu.at[:, pl.ds(256 + i * 128, 128)])
        load(f"d{i}", down_w.at[i], wdn.at[pl.ds(i * 128, 128)])

    def arrived(*names):
        for name in names:
            loads[name].wait()

    def to_ep(stage, src_of, dst_of):
        copies = []
        for j, peer in ep_peers:
            copy = pltpu.make_async_remote_copy(
                src_ref=src_of(peer),
                dst_ref=dst_of(j),
                send_sem=ep_send.at[stage, j],
                recv_sem=ep_recv.at[stage, j],
                device_id={"ep": peer},
                device_id_type=MESH_ID,
            )
            copy.start()
            copies.append(copy)
        return copies

    def to_tp(stage, src_of, dst_of):
        copies = []
        for j, peer in tp_peers:
            copy = pltpu.make_async_remote_copy(
                src_ref=src_of(peer),
                dst_ref=dst_of(j),
                send_sem=tp_send.at[stage, j],
                recv_sem=tp_recv.at[stage, j],
                device_id={"tp": peer},
                device_id_type=MESH_ID,
            )
            copy.start()
            copies.append(copy)
        return copies

    def landed(copies):
        for copy in copies:
            copy.wait_recv()

    fwt[pl.ds(16, 112), :] = jnp.zeros((112, HEAD), BF16)
    arrived("hid", "again", "fwt", "wq", "wk", "wv")
    stream = hid[...].astype(F32)
    normed = (stream * again[:, own_cols]).astype(BF16)
    projected = mm(normed, wqkv[...]).astype(BF16)
    send1[:, :, 0:512] = projected.reshape(EP, OWN, 512)
    stats = lax.dot_general(normed, fwt[...], NT, preferred_element_type=F32)
    lane = iota((SEQS, HEAD), 1)
    stats = jnp.where(lane == 16, jnp.sum(stream * stream, axis=1, keepdims=True), stats)
    high = stats.astype(BF16).astype(F32)
    low = stats - high
    both = jnp.where(lane < 64, high, pltpu.roll(low, 64, 1)).astype(BF16)
    send1[:, :, 512:640] = both.reshape(EP, OWN, HEAD)
    pl.semaphore_wait(barrier, EP + TP - 2)
    sent = to_ep(0, lambda peer: send1.at[peer], lambda j: recv1.at[j])
    first = sent

    arrived("grp", "ext", "wtt")
    chosen = [grp[...] * GROUP_EXPERTS + ext[pl.ds(k, 1), :] for k in range(2)]
    expert_row = iota((EXPERTS, SEQS), 0)
    hits = [jnp.where(expert_row == chosen[k], 1.0, 0.0) for k in range(2)]
    any_hit = hits[0] + hits[1]
    before = jnp.where(iota((SEQS, SEQS), 0) < iota((SEQS, SEQS), 1), 1.0, 0.0).astype(BF16)
    rank = mm(any_hit.astype(BF16), before)
    slot_of = rank + (expert_row * CAPACITY).astype(F32)
    slots = [
        jnp.sum(hits[k] * slot_of, axis=0, keepdims=True).astype(jnp.int32) for k in range(2)
    ]
    slot_row = iota((EXPERTS * CAPACITY, SEQS), 0)
    place[...] = jnp.where((slot_row == slots[0]) | (slot_row == slots[1]), 1.0, 0.0).astype(BF16)
    own_slot = iota((48, SEQS), 0) + e * 48
    slot_weight = jnp.sum(
        jnp.where(own_slot == slots[0], wtt[pl.ds(0, 1), :], 0.0)
        + jnp.where(own_slot == slots[1], wtt[pl.ds(1, 1), :], 0.0),
        axis=1,
        keepdims=True,
    )
    row8 = iota((8, SEQS), 0)
    slot_cols = jnp.where(row8 == 0, slots[0], slots[1]).astype(F32).T.astype(jnp.int32)
    slot_lane = iota((SEQS, EXPERTS * CAPACITY), 1)
    place_t[...] = jnp.where(
        (slot_lane == slot_cols[:, 0:1]) | (slot_lane == slot_cols[:, 1:2]), 1.0, 0.0
    ).astype(BF16)

    arrived("graw", "lens", "fbias", "qgain", "kgain")
    for b in range(OWN):
        for h in range(2):
            gates[pl.ds(h * OWN + b, 1), :] = graw[b, pl.ds(h, 1), :]
    seq_row = lax.rem(iota((2 * OWN, OWN), 0), OWN)
    len_col = jnp.sum(
        jnp.where(seq_row == iota((2 * OWN, OWN), 1), lens[...].astype(F32), 0.0),
        axis=1,
        keepdims=True,
    ).astype(jnp.int32)
    position = iota((2 * OWN, 1024), 1)
    gate_rows = gates[...]
    latest = jnp.sum(jnp.where(position == len_col - 1, gate_rows, 0.0), axis=1, keepdims=True)
    gates[...] = jnp.where(position < len_col, -gate_rows, -jnp.inf)
    lane16 = iota((1, 16), 1)
    bias = [
        jnp.sum(jnp.where(lane16 == 2 * t + h, fbias[...], 0.0), axis=1, keepdims=True)
        for h in range(2)
    ]
    for copy in kv:
        copy.wait()

    landed(first)
    sums = send1[e].astype(F32)
    for j in range(1, EP):
        sums = sums + recv1[j].astype(F32)
    stat = sums[:, 512:640]
    stat = stat + pltpu.roll(stat, 64, 1)
    lane = iota((OWN, HEAD), 1)

    def stat_at(index):
        return jnp.sum(jnp.where(lane == index, stat, 0.0), axis=1, keepdims=True)

    scale = lax.rsqrt(stat_at(16) / D + EPS)
    forget = []
    for h in range(2):
        logit = stat_at(2 * t + h) * scale + bias[h]
        forget.append(jnp.minimum(logit, 0.0) - jnp.log(1.0 + jnp.exp(-jnp.abs(logit))))

    def head_norm(rows, gain):
        mean = jnp.mean(rows * rows, axis=1, keepdims=True)
        return (rows * lax.rsqrt(mean + EPS) * gain).astype(BF16)

    queries = jnp.concatenate(
        [head_norm(sums[:, h * HEAD : (h + 1) * HEAD], qgain[...]) for h in range(2)], axis=0
    ).astype(F32)
    new_key = head_norm(sums[:, 256:384], kgain[...])
    new_value = (sums[:, 384:512] * scale).astype(BF16)
    keys_out[...] = new_key
    values_out[...] = new_value
    twice_key = jnp.concatenate([new_key, new_key], axis=0).astype(F32)
    twice_value = jnp.concatenate([new_value, new_value], axis=0).astype(F32)
    now = latest + jnp.concatenate(forget, axis=0)
    self_score = jnp.sum(queries * twice_key, axis=1, keepdims=True) * FACTOR

    q_row = lax.rem(iota((2 * OWN, HEAD), 0), OWN)
    spread = jnp.concatenate(
        [jnp.where(q_row == b, queries, 0.0).astype(BF16) for b in range(OWN)], axis=1
    )
    scores = lax.dot_general(spread, kcat[...], NT, preferred_element_type=F32)
    scores = scores * FACTOR + now + gates[...]
    ceiling = jnp.maximum(jnp.max(scores, axis=1, keepdims=True), self_score)
    weights = jnp.exp(scores - ceiling)
    self_weight = jnp.exp(self_score - ceiling)
    denominator = jnp.sum(weights, axis=1, keepdims=True) + self_weight
    p_row = lax.rem(iota((2 * OWN, 1024), 0), OWN)
    out = self_weight * twice_value
    for b in range(OWN):
        out = out + mm(jnp.where(p_row == b, weights, 0.0).astype(BF16), vbuf[b])
    out = out / denominator
    heads[e] = jnp.concatenate([out[0:OWN], out[OWN : 2 * OWN]], axis=1).astype(BF16)

    second = to_ep(1, lambda peer: heads.at[e], lambda j: heads.at[e])
    arrived("wout", "fgain", "mixv", "dg", "du", "dd", "g0", "g1", "u0", "u1", "d0", "d1")
    landed(second)
    attn = mm(heads[...].reshape(SEQS, 256), wout[...])
    own_rows = pl.ds(pl.multiple_of(t * 32, 32), 32)
    part[...] = attn
    psend[...] = attn.astype(BF16).reshape(TP, 32, HEAD)
    third = to_tp(0, lambda peer: psend.at[peer], lambda j: precv.at[j])
    landed(third)
    total = hid[own_rows, :].astype(F32) + part[own_rows, :]
    for j in range(1, TP):
        total = total + precv[j].astype(F32)
    mid[own_rows, :] = total.astype(BF16)
    fourth = to_tp(1, lambda peer: mid.at[own_rows], lambda j: mid.at[own_rows])
    landed(fourth)

    middle = mid[...]
    send4[:, 0:48, :] = mm(place[...], middle).astype(BF16).reshape(EP, 48, HEAD)
    send4[:, 48:64, :] = middle.reshape(EP, OWN, HEAD)
    rows = to_ep(2, lambda peer: send4.at[peer], lambda j: xrows.at[:, own_cols])
    normed_mid = (middle.astype(F32) * fgain[:, own_cols]).astype(BF16)
    send4d[...] = mm(normed_mid, wdense[...]).astype(BF16).reshape(EP, OWN, 1024)
    dense = to_ep(3, lambda peer: send4d.at[peer], lambda j: recv4d.at[j])
    xrows[:, own_cols] = send4[e]
    landed(rows)

    routed = xrows[0:48, :].astype(F32)
    slot_scale = lax.rsqrt(jnp.sum(routed * routed, axis=1, keepdims=True) / D + EPS)
    routed_in = (routed * fgain[...]).astype(BF16)
    both_pre = mm(routed_in, wgu[...])
    upper = iota((48, HEAD), 0) < CAPACITY
    gate_pre = jnp.where(upper, both_pre[:, 0:128], both_pre[:, 128:256]) * slot_scale
    up_pre = jnp.where(upper, both_pre[:, 256:384], both_pre[:, 384:512]) * slot_scale
    unit = silu(gate_pre) * up_pre
    units = jnp.concatenate(
        [jnp.where(upper, unit, 0.0), jnp.where(upper, 0.0, unit)], axis=1
    ).astype(BF16)
    send5[...] = (mm(units, wdn[...]) * slot_weight).astype(BF16)
    back = to_ep(
        4,
        lambda peer: send5.at[:, pl.ds(pl.multiple_of(peer * HEAD, HEAD), HEAD)],
        lambda j: ret.at[e],
    )
    ret[e] = send5[:, own_cols]

    own_mid = xrows[48:64, :].astype(F32)
    mid_scale = lax.rsqrt(jnp.sum(own_mid * own_mid, axis=1, keepdims=True) / D + EPS)
    own_normed = (own_mid * fgain[...]).astype(BF16).astype(F32)
    mix_dot = jnp.sum(own_normed * mixv[...].astype(F32), axis=1, keepdims=True)
    share = jax.nn.sigmoid(mid_scale * mix_dot)
    landed(dense)
    dsums = send4d[e].astype(F32)
    for j in range(1, EP):
        dsums = dsums + recv4d[j].astype(F32)
    dense_unit = silu(dsums[:, 0:512] * mid_scale) * (dsums[:, 512:1024] * mid_scale)
    dhid[e] = (dense_unit * share).astype(BF16)
    hidden_copies = to_ep(5, lambda peer: dhid.at[e], lambda j: dhid.at[e])

    landed(back)
    branch = mm(place_t[...], ret[...].reshape(EXPERTS * CAPACITY, HEAD))
    landed(hidden_copies)
    branch = branch + mm(dhid[...].reshape(SEQS, 512), wdd[...])
    part2[...] = branch
    psend2[...] = branch.astype(BF16).reshape(TP, 32, HEAD)
    fifth = to_tp(2, lambda peer: psend2.at[peer], lambda j: precv2.at[j])
    landed(fifth)
    total = mid[own_rows, :].astype(F32) + part2[own_rows, :]
    for j in range(1, TP):
        total = total + precv2[j].astype(F32)
    final[own_rows, :] = total.astype(BF16)
    sixth = to_tp(3, lambda peer: final.at[own_rows], lambda j: final.at[own_rows])
    landed(sixth)
    result = pltpu.make_async_copy(final, mixed_out, out_sem)
    result.start()
    for copies in (first, second, third, fourth, rows, dense, back, hidden_copies, fifth, sixth):
        for copy in copies:
            copy.wait_send()
    result.wait()


def on_device(
    hidden_in, attn_gain, forget_weight, forget_bias, query_weight, key_weight, value_weight,
    query_gain, key_gain, cache_keys, cache_values, cache_gates, lengths, output_weight,
    ffn_gain, route_group, route_expert, route_weight, expert_gate, expert_up, expert_down,
    mix_vector, dense_gate, dense_up, dense_down,
):
    vmem = pltpu.VMEM
    anywhere = pl.BlockSpec(memory_space=pl.ANY)
    scratch = [
        vmem((SEQS, HEAD), BF16),
        vmem((1, D), F32),
        vmem((HEAD, HEAD), BF16),
        vmem((1, 16), F32),
        vmem((HEAD, 512), BF16),
        vmem((1, HEAD), F32),
        vmem((1, HEAD), F32),
        vmem((1024, OWN * HEAD), BF16),
        vmem((OWN, 1024, HEAD), BF16),
        vmem((OWN, 2, 1024), F32),
        vmem((1, OWN), jnp.int32),
        vmem((256, HEAD), BF16),
        vmem((1, D), F32),
        vmem((1, SEQS), jnp.int32),
        vmem((2, SEQS), jnp.int32),
        vmem((2, SEQS), F32),
        vmem((D, 512), BF16),
        vmem((256, D), BF16),
        vmem((1, D), BF16),
        vmem((HEAD, 1024), BF16),
        vmem((512, HEAD), BF16),
        vmem((EP, OWN, 640), BF16),
        vmem((EP, OWN, 640), BF16),
        vmem((2 * OWN, 1024), F32),
        vmem((EXPERTS * CAPACITY, SEQS), BF16),
        vmem((SEQS, EXPERTS * CAPACITY), BF16),
        vmem((EP, OWN, 256), BF16),
        vmem((SEQS, HEAD), F32),
        vmem((TP, 32, HEAD), BF16),
        vmem((TP, 32, HEAD), BF16),
        vmem((SEQS, HEAD), BF16),
        vmem((EP, 64, HEAD), BF16),
        vmem((64, D), BF16),
        vmem((EP, OWN, 1024), BF16),
        vmem((EP, OWN, 1024), BF16),
        vmem((48, D), BF16),
        vmem((EP, 48, HEAD), BF16),
        vmem((EP, OWN, 512), BF16),
        vmem((SEQS, HEAD), F32),
        vmem((TP, 32, HEAD), BF16),
        vmem((TP, 32, HEAD), BF16),
        vmem((SEQS, HEAD), BF16),
        pltpu.SemaphoreType.DMA((26,)),
        pltpu.SemaphoreType.DMA((2, OWN)),
        pltpu.SemaphoreType.DMA((6, EP)),
        pltpu.SemaphoreType.DMA((6, EP)),
        pltpu.SemaphoreType.DMA((4, TP)),
        pltpu.SemaphoreType.DMA((4, TP)),
        pltpu.SemaphoreType.DMA,
    ]
    call = pl.pallas_call(
        layer,
        out_shape=(
            jax.ShapeDtypeStruct((SEQS, HEAD), BF16),
            jax.ShapeDtypeStruct((OWN, HEAD), BF16),
            jax.ShapeDtypeStruct((OWN, HEAD), BF16),
        ),
        in_specs=[anywhere] * 25,
        out_specs=(
            anywhere,
            pl.BlockSpec(memory_space=pltpu.VMEM),
            pl.BlockSpec(memory_space=pltpu.VMEM),
        ),
        scratch_shapes=scratch,
        compiler_params=pltpu.CompilerParams(
            collective_id=0, has_side_effects=True, vmem_limit_bytes=60 * 1024 * 1024
        ),
    )
    return call(
        hidden_in,
        attn_gain.reshape(1, D),
        forget_weight.T,
        forget_bias.reshape(1, 16),
        query_weight,
        key_weight,
        value_weight,
        query_gain.reshape(1, HEAD),
        key_gain.reshape(1, HEAD),
        cache_keys.reshape(OWN, 1024, HEAD),
        cache_values.reshape(OWN, 1024, HEAD),
        cache_gates,
        lengths.reshape(1, OWN),
        output_weight,
        ffn_gain.reshape(1, D),
        route_group.reshape(1, SEQS),
        route_expert.T,
        route_weight.T,
        expert_gate,
        expert_up,
        expert_down,
        mix_vector.reshape(1, D),
        dense_gate,
        dense_up,
        dense_down,
    )


def solution(mesh):
    placed = (
        P(None, "ep"), P(), P(), P(), P("ep", "tp"), P("ep", "tp"), P("ep", "tp"), P(), P(),
        P("ep", "tp", None, None), P("ep", "tp", None, None), P("ep", "tp", None), P("ep"),
        P("tp", "ep"), P(), P(), P(), P(), P("ep", None, "tp"), P("ep", None, "tp"),
        P("ep", "tp", None), P(), P("ep", "tp"), P("ep", "tp"), P("tp", "ep"),
    )
    return jax.shard_map(
        on_device,
        mesh=mesh,
        in_specs=placed,
        out_specs=(P(None, "ep"), P("ep", "tp"), P("ep", "tp")),
        check_vma=False,
    )
```

```python
import jax
import jax.numpy as jnp
from jax import lax
from jax.experimental import pallas as pl
from jax.experimental.pallas import tpu as pltpu
from jax.sharding import PartitionSpec as P

D = 2048
HEAD = 128
GROUP_EXPERTS = 4
CAPACITY = 24
EXPERTS = 32
SEQS = 256
EP = 16
TP = 8
OWN = SEQS // EP
CHUNKS = 2
WIDE = 512 // CHUNKS
EPS = 1e-06
FACTOR = HEAD**-0.5
F32 = jnp.float32
BF16 = jnp.bfloat16
MESH_ID = pl.DeviceIdType.MESH
NT = (((1,), (1,)), ((), ()))

EP_OFFSETS = sorted(
    [(dz, dx) for dz in range(4) for dx in range(4) if (dz, dx) != (0, 0)],
    key=lambda o: -(min(o[0], 4 - o[0]) + min(o[1], 4 - o[1])),
)
TP_OFFSETS = [4, 5, 3, 2, 6, 7, 1]


def mm(a, b):
    return jnp.dot(a, b, preferred_element_type=F32)


def iota(shape, dim):
    return lax.broadcasted_iota(jnp.int32, shape, dim)


def silu(v):
    return v * jax.nn.sigmoid(v)


def put_out(mixed, keys, values, mixed_out, keys_out, values_out, sems):
    copies = [
        pltpu.make_async_copy(src, dst, sems.at[i])
        for i, (src, dst) in enumerate(
            ((mixed, mixed_out), (keys, keys_out), (values, values_out))
        )
    ]
    for copy in copies:
        copy.start()
    for copy in copies:
        copy.wait()


def layer(
    hidden, attn_gain, forget_t, forget_bias, query_w, key_w, value_w, query_gain, key_gain,
    cache_k, cache_v, cache_g, lengths, output_w, ffn_gain, group, expert_t, weight_t,
    gate_w, up_w, down_w, mix_vector, dense_gate, dense_up, dense_down,
    mixed_out, keys_out, values_out,
    hid, again, fwt, fbias, wqkv, qgain, kgain, kcat, vbuf, graw, lens, wout, fgain,
    grp, ext, wtt, wgu, wdn, mixv, wdense, wdd,
    send1, recv1, gates, place, place_t, heads, part, psend, precv, mid,
    send4, xrows, send4d, recv4d, send5, ret, dhid, part2, psend2, precv2, final,
    load_sem, kv_sem, ep_send, ep_recv, tp_send, tp_recv,
):
    e = lax.axis_index("ep")
    t = lax.axis_index("tp")
    z = lax.div(e, 4)
    x = lax.rem(e, 4)
    ep_peers = [
        (dz * 4 + dx, lax.rem(z + dz, 4) * 4 + lax.rem(x + dx, 4)) for dz, dx in EP_OFFSETS
    ]
    tp_peers = [(j, lax.rem(t + j, TP)) for j in TP_OFFSETS]
    own_cols = pl.ds(pl.multiple_of(e * HEAD, HEAD), HEAD)

    barrier = pltpu.get_barrier_semaphore()
    for _, peer in ep_peers:
        pl.semaphore_signal(barrier, inc=1, device_id={"ep": peer}, device_id_type=MESH_ID)
    for _, peer in tp_peers:
        pl.semaphore_signal(barrier, inc=1, device_id={"tp": peer}, device_id_type=MESH_ID)

    loads = {}

    def load(name, src, dst):
        copy = pltpu.make_async_copy(src, dst, load_sem.at[len(loads)])
        copy.start()
        loads[name] = copy

    load("hid", hidden, hid)
    load("again", attn_gain, again)
    load("fwt", forget_t.at[:, own_cols], fwt.at[pl.ds(0, 16)])
    load("wq", query_w, wqkv.at[:, pl.ds(0, 256)])
    load("wk", key_w, wqkv.at[:, pl.ds(256, 128)])
    load("wv", value_w, wqkv.at[:, pl.ds(384, 128)])
    load("grp", group, grp)
    load("ext", expert_t, ext)
    load("wtt", weight_t, wtt)
    load("graw", cache_g, graw)
    load("lens", lengths, lens)
    load("fbias", forget_bias, fbias)
    load("qgain", query_gain, qgain)
    load("kgain", key_gain, kgain)
    kv = []
    for b in range(OWN):
        copy = pltpu.make_async_copy(
            cache_k.at[b], kcat.at[:, pl.ds(b * HEAD, HEAD)], kv_sem.at[0, b]
        )
        copy.start()
        kv.append(copy)
    for b in range(OWN):
        copy = pltpu.make_async_copy(cache_v.at[b], vbuf.at[b], kv_sem.at[1, b])
        copy.start()
        kv.append(copy)
    load("wout", output_w, wout)
    load("fgain", ffn_gain, fgain)
    load("mixv", mix_vector, mixv)
    for c in range(CHUNKS):
        cols = pl.ds(c * WIDE, WIDE)
        load(f"dg{c}", dense_gate.at[:, cols], wdense.at[:, pl.ds(2 * c * WIDE, WIDE)])
        load(f"du{c}", dense_up.at[:, cols], wdense.at[:, pl.ds((2 * c + 1) * WIDE, WIDE)])
    load("dd", dense_down, wdd)
    for i in range(2):
        load(f"g{i}", gate_w.at[i], wgu.at[:, pl.ds(i * 128, 128)])
        load(f"u{i}", up_w.at[i], wgu.at[:, pl.ds(256 + i * 128, 128)])
        load(f"d{i}", down_w.at[i], wdn.at[pl.ds(i * 128, 128)])

    def arrived(*names):
        for name in names:
            loads[name].wait()

    def to_ep(stage, src_of, dst_of):
        copies = []
        for j, peer in ep_peers:
            copy = pltpu.make_async_remote_copy(
                src_ref=src_of(peer),
                dst_ref=dst_of(j),
                send_sem=ep_send.at[stage, j],
                recv_sem=ep_recv.at[stage, j],
                device_id={"ep": peer},
                device_id_type=MESH_ID,
            )
            copy.start()
            copies.append(copy)
        return copies

    def to_tp(stage, src_of, dst_of):
        copies = []
        for j, peer in tp_peers:
            copy = pltpu.make_async_remote_copy(
                src_ref=src_of(peer),
                dst_ref=dst_of(j),
                send_sem=tp_send.at[stage, j],
                recv_sem=tp_recv.at[stage, j],
                device_id={"tp": peer},
                device_id_type=MESH_ID,
            )
            copy.start()
            copies.append(copy)
        return copies

    def landed(copies):
        for copy in copies:
            copy.wait_recv()

    fwt[pl.ds(16, 112), :] = jnp.zeros((112, HEAD), BF16)
    arrived("hid", "again", "fwt", "wq", "wk", "wv")
    stream = hid[...].astype(F32)
    normed = (stream * again[:, own_cols]).astype(BF16)
    projected = mm(normed, wqkv[...]).astype(BF16)
    send1[:, :, 0:512] = projected.reshape(EP, OWN, 512)
    stats = lax.dot_general(normed, fwt[...], NT, preferred_element_type=F32)
    lane = iota((SEQS, HEAD), 1)
    stats = jnp.where(lane == 16, jnp.sum(stream * stream, axis=1, keepdims=True), stats)
    high = stats.astype(BF16).astype(F32)
    low = stats - high
    both = jnp.where(lane < 64, high, pltpu.roll(low, 64, 1)).astype(BF16)
    send1[:, :, 512:640] = both.reshape(EP, OWN, HEAD)
    pl.semaphore_wait(barrier, EP + TP - 2)
    sent = to_ep(0, lambda peer: send1.at[peer], lambda j: recv1.at[j])
    first = sent

    arrived("grp", "ext", "wtt")
    chosen = [grp[...] * GROUP_EXPERTS + ext[pl.ds(k, 1), :] for k in range(2)]
    expert_row = iota((EXPERTS, SEQS), 0)
    hits = [jnp.where(expert_row == chosen[k], 1.0, 0.0) for k in range(2)]
    any_hit = hits[0] + hits[1]
    before = jnp.where(iota((SEQS, SEQS), 0) < iota((SEQS, SEQS), 1), 1.0, 0.0).astype(BF16)
    rank = mm(any_hit.astype(BF16), before)
    slot_of = rank + (expert_row * CAPACITY).astype(F32)
    slots = [
        jnp.sum(hits[k] * slot_of, axis=0, keepdims=True).astype(jnp.int32) for k in range(2)
    ]
    slot_row = iota((EXPERTS * CAPACITY, SEQS), 0)
    place[...] = jnp.where((slot_row == slots[0]) | (slot_row == slots[1]), 1.0, 0.0).astype(BF16)
    own_slot = iota((48, SEQS), 0) + e * 48
    slot_weight = jnp.sum(
        jnp.where(own_slot == slots[0], wtt[pl.ds(0, 1), :], 0.0)
        + jnp.where(own_slot == slots[1], wtt[pl.ds(1, 1), :], 0.0),
        axis=1,
        keepdims=True,
    )
    row8 = iota((8, SEQS), 0)
    slot_cols = jnp.where(row8 == 0, slots[0], slots[1]).astype(F32).T.astype(jnp.int32)
    slot_lane = iota((SEQS, EXPERTS * CAPACITY), 1)
    place_t[...] = jnp.where(
        (slot_lane == slot_cols[:, 0:1]) | (slot_lane == slot_cols[:, 1:2]), 1.0, 0.0
    ).astype(BF16)

    arrived("graw", "lens", "fbias", "qgain", "kgain")
    for b in range(OWN):
        for h in range(2):
            gates[pl.ds(h * OWN + b, 1), :] = graw[b, pl.ds(h, 1), :]
    seq_row = lax.rem(iota((2 * OWN, OWN), 0), OWN)
    len_col = jnp.sum(
        jnp.where(seq_row == iota((2 * OWN, OWN), 1), lens[...].astype(F32), 0.0),
        axis=1,
        keepdims=True,
    ).astype(jnp.int32)
    position = iota((2 * OWN, 1024), 1)
    gate_rows = gates[...]
    latest = jnp.sum(jnp.where(position == len_col - 1, gate_rows, 0.0), axis=1, keepdims=True)
    gates[...] = jnp.where(position < len_col, -gate_rows, -jnp.inf)
    lane16 = iota((1, 16), 1)
    bias = [
        jnp.sum(jnp.where(lane16 == 2 * t + h, fbias[...], 0.0), axis=1, keepdims=True)
        for h in range(2)
    ]
    for copy in kv:
        copy.wait()

    landed(first)
    sums = send1[e].astype(F32)
    for j in range(1, EP):
        sums = sums + recv1[j].astype(F32)
    stat = sums[:, 512:640]
    stat = stat + pltpu.roll(stat, 64, 1)
    lane = iota((OWN, HEAD), 1)

    def stat_at(index):
        return jnp.sum(jnp.where(lane == index, stat, 0.0), axis=1, keepdims=True)

    scale = lax.rsqrt(stat_at(16) / D + EPS)
    forget = []
    for h in range(2):
        logit = stat_at(2 * t + h) * scale + bias[h]
        forget.append(jnp.minimum(logit, 0.0) - jnp.log(1.0 + jnp.exp(-jnp.abs(logit))))

    def head_norm(rows, gain):
        mean = jnp.mean(rows * rows, axis=1, keepdims=True)
        return (rows * lax.rsqrt(mean + EPS) * gain).astype(BF16)

    queries = jnp.concatenate(
        [head_norm(sums[:, h * HEAD : (h + 1) * HEAD], qgain[...]) for h in range(2)], axis=0
    ).astype(F32)
    new_key = head_norm(sums[:, 256:384], kgain[...])
    new_value = (sums[:, 384:512] * scale).astype(BF16)
    keys_out[...] = new_key
    values_out[...] = new_value
    twice_key = jnp.concatenate([new_key, new_key], axis=0).astype(F32)
    twice_value = jnp.concatenate([new_value, new_value], axis=0).astype(F32)
    now = latest + jnp.concatenate(forget, axis=0)
    self_score = jnp.sum(queries * twice_key, axis=1, keepdims=True) * FACTOR

    q_row = lax.rem(iota((2 * OWN, HEAD), 0), OWN)
    spread = jnp.concatenate(
        [jnp.where(q_row == b, queries, 0.0).astype(BF16) for b in range(OWN)], axis=1
    )
    scores = lax.dot_general(spread, kcat[...], NT, preferred_element_type=F32)
    scores = scores * FACTOR + now + gates[...]
    ceiling = jnp.maximum(jnp.max(scores, axis=1, keepdims=True), self_score)
    weights = jnp.exp(scores - ceiling)
    self_weight = jnp.exp(self_score - ceiling)
    denominator = jnp.sum(weights, axis=1, keepdims=True) + self_weight
    p_row = lax.rem(iota((2 * OWN, 1024), 0), OWN)
    out = self_weight * twice_value
    for b in range(OWN):
        out = out + mm(jnp.where(p_row == b, weights, 0.0).astype(BF16), vbuf[b])
    out = out / denominator
    heads[e] = jnp.concatenate([out[0:OWN], out[OWN : 2 * OWN]], axis=1).astype(BF16)

    second = to_ep(1, lambda peer: heads.at[e], lambda j: heads.at[e])
    arrived("wout", "fgain", "mixv", "dd", "g0", "g1", "u0", "u1", "d0", "d1")
    arrived(*[f"dg{c}" for c in range(CHUNKS)], *[f"du{c}" for c in range(CHUNKS)])
    landed(second)
    attn = mm(heads[...].reshape(SEQS, 256), wout[...])
    own_rows = pl.ds(pl.multiple_of(t * 32, 32), 32)
    part[...] = attn
    psend[...] = attn.astype(BF16).reshape(TP, 32, HEAD)
    third = to_tp(0, lambda peer: psend.at[peer], lambda j: precv.at[j])
    landed(third)
    total = hid[own_rows, :].astype(F32) + part[own_rows, :]
    for j in range(1, TP):
        total = total + precv[j].astype(F32)
    mid[own_rows, :] = total.astype(BF16)
    fourth = to_tp(1, lambda peer: mid.at[own_rows], lambda j: mid.at[own_rows])
    landed(fourth)

    middle = mid[...]
    send4[:, 0:48, :] = mm(place[...], middle).astype(BF16).reshape(EP, 48, HEAD)
    send4[:, 48:64, :] = middle.reshape(EP, OWN, HEAD)
    rows = to_ep(2, lambda peer: send4.at[peer], lambda j: xrows.at[:, own_cols])
    normed_mid = (middle.astype(F32) * fgain[:, own_cols]).astype(BF16)
    dense = []
    for c in range(CHUNKS):
        dense_part = mm(normed_mid, wdense[:, 2 * c * WIDE : 2 * (c + 1) * WIDE])
        send4d[c] = dense_part.astype(BF16).reshape(EP, OWN, 2 * WIDE)
        dense.append(
            to_ep(5 + c, lambda peer: send4d.at[c, peer], lambda j: recv4d.at[c, j])
        )
    xrows[:, own_cols] = send4[e]
    landed(rows)

    routed = xrows[0:48, :].astype(F32)
    slot_scale = lax.rsqrt(jnp.sum(routed * routed, axis=1, keepdims=True) / D + EPS)
    routed_in = (routed * fgain[...]).astype(BF16)
    both_pre = mm(routed_in, wgu[...])
    upper = iota((48, HEAD), 0) < CAPACITY
    gate_pre = jnp.where(upper, both_pre[:, 0:128], both_pre[:, 128:256]) * slot_scale
    up_pre = jnp.where(upper, both_pre[:, 256:384], both_pre[:, 384:512]) * slot_scale
    unit = silu(gate_pre) * up_pre
    units = jnp.concatenate(
        [jnp.where(upper, unit, 0.0), jnp.where(upper, 0.0, unit)], axis=1
    ).astype(BF16)
    send5[...] = (mm(units, wdn[...]) * slot_weight).astype(BF16)
    back = to_ep(
        3,
        lambda peer: send5.at[:, pl.ds(pl.multiple_of(peer * HEAD, HEAD), HEAD)],
        lambda j: ret.at[e],
    )
    ret[e] = send5[:, own_cols]

    own_mid = xrows[48:64, :].astype(F32)
    mid_scale = lax.rsqrt(jnp.sum(own_mid * own_mid, axis=1, keepdims=True) / D + EPS)
    own_normed = (own_mid * fgain[...]).astype(BF16).astype(F32)
    mix_rows = mixv[...].astype(F32)
    mix_dot = sum(
        own_normed[:, s * HEAD : (s + 1) * HEAD] * mix_rows[s : s + 1] for s in range(EP)
    ).sum(axis=1, keepdims=True)
    share = jax.nn.sigmoid(mid_scale * mix_dot)
    hidden_copies = []
    for c in range(CHUNKS):
        landed(dense[c])
        dsums = send4d[c, e].astype(F32)
        for j in range(1, EP):
            dsums = dsums + recv4d[c, j].astype(F32)
        dense_unit = silu(dsums[:, :WIDE] * mid_scale) * (dsums[:, WIDE:] * mid_scale)
        dhid[c, e] = (dense_unit * share).astype(BF16)
        hidden_copies.append(
            to_ep(5 + CHUNKS + c, lambda peer: dhid.at[c, e], lambda j: dhid.at[c, e])
        )

    landed(back)
    branch = mm(place_t[...], ret[...].reshape(EXPERTS * CAPACITY, HEAD))
    for c in range(CHUNKS):
        landed(hidden_copies[c])
        branch = branch + mm(
            dhid[c].reshape(SEQS, WIDE), wdd[c * WIDE : (c + 1) * WIDE, :]
        )
    part2[...] = branch
    psend2[...] = branch.astype(BF16).reshape(TP, 32, HEAD)
    fifth = to_tp(2, lambda peer: psend2.at[peer], lambda j: precv2.at[j])
    landed(fifth)
    total = mid[own_rows, :].astype(F32) + part2[own_rows, :]
    for j in range(1, TP):
        total = total + precv2[j].astype(F32)
    final[own_rows, :] = total.astype(BF16)
    sixth = to_tp(3, lambda peer: final.at[own_rows], lambda j: final.at[own_rows])
    landed(sixth)
    mixed_out[...] = final[...]
    groups = [first, second, third, fourth, rows, back, fifth, sixth]
    for copies in groups + dense + hidden_copies:
        for copy in copies:
            copy.wait_send()


def on_device(
    hidden_in, attn_gain, forget_weight, forget_bias, query_weight, key_weight, value_weight,
    query_gain, key_gain, cache_keys, cache_values, cache_gates, lengths, output_weight,
    ffn_gain, route_group, route_expert, route_weight, expert_gate, expert_up, expert_down,
    mix_vector, dense_gate, dense_up, dense_down,
):
    vmem = pltpu.VMEM
    anywhere = pl.BlockSpec(memory_space=pltpu.HBM)
    scratch = [
        vmem((SEQS, HEAD), BF16),
        vmem((1, D), F32),
        vmem((HEAD, HEAD), BF16),
        vmem((1, 16), F32),
        vmem((HEAD, 512), BF16),
        vmem((1, HEAD), F32),
        vmem((1, HEAD), F32),
        vmem((1024, OWN * HEAD), BF16),
        vmem((OWN, 1024, HEAD), BF16),
        vmem((OWN, 2, 1024), F32),
        vmem((1, OWN), jnp.int32),
        vmem((256, HEAD), BF16),
        vmem((1, D), F32),
        vmem((1, SEQS), jnp.int32),
        vmem((2, SEQS), jnp.int32),
        vmem((2, SEQS), F32),
        vmem((D, 512), BF16),
        vmem((256, D), BF16),
        vmem((16, HEAD), BF16),
        vmem((HEAD, 1024), BF16),
        vmem((512, HEAD), BF16),
        vmem((EP, OWN, 640), BF16),
        vmem((EP, OWN, 640), BF16),
        vmem((2 * OWN, 1024), F32),
        vmem((EXPERTS * CAPACITY, SEQS), BF16),
        vmem((SEQS, EXPERTS * CAPACITY), BF16),
        vmem((EP, OWN, 256), BF16),
        vmem((SEQS, HEAD), F32),
        vmem((TP, 32, HEAD), BF16),
        vmem((TP, 32, HEAD), BF16),
        vmem((SEQS, HEAD), BF16),
        vmem((EP, 64, HEAD), BF16),
        vmem((64, D), BF16),
        vmem((CHUNKS, EP, OWN, 2 * WIDE), BF16),
        vmem((CHUNKS, EP, OWN, 2 * WIDE), BF16),
        vmem((48, D), BF16),
        vmem((EP, 48, HEAD), BF16),
        vmem((CHUNKS, EP, OWN, WIDE), BF16),
        vmem((SEQS, HEAD), F32),
        vmem((TP, 32, HEAD), BF16),
        vmem((TP, 32, HEAD), BF16),
        vmem((SEQS, HEAD), BF16),
        pltpu.SemaphoreType.DMA((24 + 2 * CHUNKS,)),
        pltpu.SemaphoreType.DMA((2, OWN)),
        pltpu.SemaphoreType.DMA((5 + 2 * CHUNKS, EP)),
        pltpu.SemaphoreType.DMA((5 + 2 * CHUNKS, EP)),
        pltpu.SemaphoreType.DMA((4, TP)),
        pltpu.SemaphoreType.DMA((4, TP)),
    ]
    call = pl.pallas_call(
        layer,
        out_shape=(
            vmem((SEQS, HEAD), BF16),
            vmem((OWN, HEAD), BF16),
            vmem((OWN, HEAD), BF16),
        ),
        in_specs=[anywhere] * 25,
        out_specs=(pl.BlockSpec(memory_space=pltpu.VMEM),) * 3,
        scratch_shapes=scratch,
        compiler_params=pltpu.CompilerParams(
            collective_id=0, has_side_effects=True, vmem_limit_bytes=60 * 1024 * 1024
        ),
    )
    results = call(
        hidden_in,
        attn_gain.reshape(1, D),
        forget_weight.T,
        forget_bias.reshape(1, 16),
        query_weight,
        key_weight,
        value_weight,
        query_gain.reshape(1, HEAD),
        key_gain.reshape(1, HEAD),
        cache_keys.reshape(OWN, 1024, HEAD),
        cache_values.reshape(OWN, 1024, HEAD),
        cache_gates,
        lengths.reshape(1, OWN),
        output_weight,
        ffn_gain.reshape(1, D),
        route_group.reshape(1, SEQS),
        route_expert.T,
        route_weight.T,
        expert_gate,
        expert_up,
        expert_down,
        mix_vector.reshape(16, HEAD),
        dense_gate,
        dense_up,
        dense_down,
    )
    return pl.pallas_call(
        put_out,
        out_shape=[jax.ShapeDtypeStruct(r.shape, r.dtype) for r in results],
        in_specs=[pl.BlockSpec(memory_space=pltpu.VMEM)] * 3,
        out_specs=[anywhere] * 3,
        scratch_shapes=[pltpu.SemaphoreType.DMA((3,))],
        compiler_params=pltpu.CompilerParams(vmem_limit_bytes=1024 * 1024),
    )(*results)


def solution(mesh):
    placed = (
        P(None, "ep"), P(), P(), P(), P("ep", "tp"), P("ep", "tp"), P("ep", "tp"), P(), P(),
        P("ep", "tp", None, None), P("ep", "tp", None, None), P("ep", "tp", None), P("ep"),
        P("tp", "ep"), P(), P(), P(), P(), P("ep", None, "tp"), P("ep", None, "tp"),
        P("ep", "tp", None), P(), P("ep", "tp"), P("ep", "tp"), P("tp", "ep"),
    )
    return jax.shard_map(
        on_device,
        mesh=mesh,
        in_specs=placed,
        out_specs=(P(None, "ep"), P("ep", "tp"), P("ep", "tp")),
        check_vma=False,
    )
```

```python
import jax
import jax.numpy as jnp
from jax import lax
from jax.experimental import pallas as pl
from jax.experimental.pallas import tpu as pltpu
from jax.sharding import PartitionSpec as P

D = 2048
HEAD = 128
GROUP_EXPERTS = 4
CAPACITY = 24
EXPERTS = 32
SEQS = 256
EP = 16
OWN = SEQS // EP
CHUNKS = 2
WIDE = 512 // CHUNKS
EPS = 1e-06
FACTOR = HEAD**-0.5
F32 = jnp.float32
BF16 = jnp.bfloat16
MESH_ID = pl.DeviceIdType.MESH
NT = (((1,), (1,)), ((), ()))

EP_OFFSETS = sorted(
    [(dz, dx) for dz in range(4) for dx in range(4) if (dz, dx) != (0, 0)],
    key=lambda o: -(min(o[0], 4 - o[0]) + min(o[1], 4 - o[1])),
)


def mm(a, b):
    return jnp.dot(a, b, preferred_element_type=F32)


def iota(shape, dim):
    return lax.broadcasted_iota(jnp.int32, shape, dim)


def silu(v):
    return v * jax.nn.sigmoid(v)


def put_out(mixed, keys, values, mixed_out, keys_out, values_out, sems):
    copies = [
        pltpu.make_async_copy(src, dst, sems.at[i])
        for i, (src, dst) in enumerate(
            ((mixed, mixed_out), (keys, keys_out), (values, values_out))
        )
    ]
    for copy in copies:
        copy.start()
    for copy in copies:
        copy.wait()


def layer(
    hidden, attn_gain, forget_t, forget_bias, query_w, key_w, value_w, query_gain, key_gain,
    cache_k, cache_v, cache_g, lengths, output_w, ffn_gain, group, expert_t, weight_t,
    gate_w, up_w, down_w, mix_vector, dense_gate, dense_up, dense_down,
    mixed_out, keys_out, values_out,
    hid, again, fwt, fbias, wqkv, qgain, kgain, kcat, vbuf, graw, lens, wout, fgain,
    grp, ext, wtt, wgu, wdn, mixv, wdense, wdd,
    send1, recv1, gates, place, place_t, heads, halves, other, chips, mid,
    send4, xrows, send4d, recv4d, send5, ret, dhid, halves2, other2, chips2, final,
    load_sem, kv_sem, ep_send, ep_recv, tp_send, tp_recv,
):
    e = lax.axis_index("ep")
    t = lax.axis_index("tp")
    z = lax.div(e, 4)
    x = lax.rem(e, 4)
    ep_peers = [
        (dz * 4 + dx, lax.rem(z + dz, 4) * 4 + lax.rem(x + dx, 4)) for dz, dx in EP_OFFSETS
    ]
    y = lax.div(t, 2)
    core = lax.rem(t, 2)
    sibling = t + 1 - 2 * core
    y_peers = [(j, lax.rem(y + j, 4) * 2 + core) for j in (2, 1, 3)]
    own_cols = pl.ds(pl.multiple_of(e * HEAD, HEAD), HEAD)

    barrier = pltpu.get_barrier_semaphore()
    for _, peer in ep_peers:
        pl.semaphore_signal(barrier, inc=1, device_id={"ep": peer}, device_id_type=MESH_ID)
    for peer in [peer for _, peer in y_peers] + [sibling]:
        pl.semaphore_signal(barrier, inc=1, device_id={"tp": peer}, device_id_type=MESH_ID)

    loads = {}

    def load(name, src, dst):
        copy = pltpu.make_async_copy(src, dst, load_sem.at[len(loads)])
        copy.start()
        loads[name] = copy

    load("hid", hidden, hid)
    load("again", attn_gain, again)
    load("fwt", forget_t.at[:, own_cols], fwt.at[pl.ds(0, 16)])
    load("wq", query_w, wqkv.at[:, pl.ds(0, 256)])
    load("wk", key_w, wqkv.at[:, pl.ds(256, 128)])
    load("wv", value_w, wqkv.at[:, pl.ds(384, 128)])
    load("grp", group, grp)
    load("ext", expert_t, ext)
    load("wtt", weight_t, wtt)
    load("graw", cache_g, graw)
    load("lens", lengths, lens)
    load("fbias", forget_bias, fbias)
    load("qgain", query_gain, qgain)
    load("kgain", key_gain, kgain)
    kv = []
    for b in range(OWN):
        copy = pltpu.make_async_copy(
            cache_k.at[b], kcat.at[:, pl.ds(b * HEAD, HEAD)], kv_sem.at[0, b]
        )
        copy.start()
        kv.append(copy)
    for b in range(OWN):
        copy = pltpu.make_async_copy(cache_v.at[b], vbuf.at[b], kv_sem.at[1, b])
        copy.start()
        kv.append(copy)
    load("wout", output_w, wout)
    load("fgain", ffn_gain, fgain)
    load("mixv", mix_vector, mixv)
    for c in range(CHUNKS):
        cols = pl.ds(c * WIDE, WIDE)
        load(f"dg{c}", dense_gate.at[:, cols], wdense.at[:, pl.ds(2 * c * WIDE, WIDE)])
        load(f"du{c}", dense_up.at[:, cols], wdense.at[:, pl.ds((2 * c + 1) * WIDE, WIDE)])
    load("dd", dense_down, wdd)
    for i in range(2):
        load(f"g{i}", gate_w.at[i], wgu.at[:, pl.ds(i * 128, 128)])
        load(f"u{i}", up_w.at[i], wgu.at[:, pl.ds(256 + i * 128, 128)])
        load(f"d{i}", down_w.at[i], wdn.at[pl.ds(i * 128, 128)])

    def arrived(*names):
        for name in names:
            loads[name].wait()

    def to_ep(stage, src_of, dst_of):
        copies = []
        for j, peer in ep_peers:
            copy = pltpu.make_async_remote_copy(
                src_ref=src_of(peer),
                dst_ref=dst_of(j),
                send_sem=ep_send.at[stage, j],
                recv_sem=ep_recv.at[stage, j],
                device_id={"ep": peer},
                device_id_type=MESH_ID,
            )
            copy.start()
            copies.append(copy)
        return copies

    def to_tp(peer, src, dst, index):
        copy = pltpu.make_async_remote_copy(
            src_ref=src,
            dst_ref=dst,
            send_sem=tp_send.at[index],
            recv_sem=tp_recv.at[index],
            device_id={"tp": peer},
            device_id_type=MESH_ID,
        )
        copy.start()
        return copy

    def landed(copies):
        for copy in copies:
            copy.wait_recv()

    half = pl.ds(pl.multiple_of(core * 128, 128), 128)
    tp_copies = []

    def add_over_tp(stage, terms, base, halves, other, chips, dst):
        halves[...] = terms.reshape(2, 128, HEAD)
        pair = to_tp(sibling, halves.at[1 - core], other, 5 * stage)
        pair.wait_recv()
        chips[y] = (halves[core] + other[...]).astype(BF16)
        along = [
            to_tp(peer, chips.at[y], chips.at[y], 5 * stage + j) for j, peer in y_peers
        ]
        landed(along)
        total = base[half, :].astype(F32)
        for chip in range(4):
            total = total + chips[chip].astype(F32)
        dst[half, :] = total.astype(BF16)
        last = to_tp(sibling, dst.at[half], dst.at[half], 5 * stage + 4)
        last.wait_recv()
        tp_copies.extend([pair, last, *along])

    fwt[pl.ds(16, 112), :] = jnp.zeros((112, HEAD), BF16)
    arrived("hid", "again", "fwt", "wq", "wk", "wv")
    stream = hid[...].astype(F32)
    normed = (stream * again[:, own_cols]).astype(BF16)
    projected = mm(normed, wqkv[...]).astype(BF16)
    send1[:, :, 0:512] = projected.reshape(EP, OWN, 512)
    stats = lax.dot_general(normed, fwt[...], NT, preferred_element_type=F32)
    lane = iota((SEQS, HEAD), 1)
    stats = jnp.where(lane == 16, jnp.sum(stream * stream, axis=1, keepdims=True), stats)
    high = stats.astype(BF16).astype(F32)
    low = stats - high
    both = jnp.where(lane < 64, high, pltpu.roll(low, 64, 1)).astype(BF16)
    send1[:, :, 512:640] = both.reshape(EP, OWN, HEAD)
    pl.semaphore_wait(barrier, EP - 1 + 4)
    sent = to_ep(0, lambda peer: send1.at[peer], lambda j: recv1.at[j])
    first = sent

    arrived("grp", "ext", "wtt")
    chosen = [grp[...] * GROUP_EXPERTS + ext[pl.ds(k, 1), :] for k in range(2)]
    expert_row = iota((EXPERTS, SEQS), 0)
    hits = [jnp.where(expert_row == chosen[k], 1.0, 0.0) for k in range(2)]
    any_hit = hits[0] + hits[1]
    before = jnp.where(iota((SEQS, SEQS), 0) < iota((SEQS, SEQS), 1), 1.0, 0.0).astype(BF16)
    rank = mm(any_hit.astype(BF16), before)
    slot_of = rank + (expert_row * CAPACITY).astype(F32)
    slots = [
        jnp.sum(hits[k] * slot_of, axis=0, keepdims=True).astype(jnp.int32) for k in range(2)
    ]
    three = (EP, CAPACITY, SEQS)
    slot_row = (2 * iota(three, 0) + core) * CAPACITY + iota(three, 1)
    hit = (slot_row == slots[0][None]) | (slot_row == slots[1][None])
    place[...] = jnp.where(hit, 1.0, 0.0).reshape(EP * CAPACITY, SEQS).astype(BF16)
    own_slot = iota((48, SEQS), 0) + e * 48
    slot_weight = jnp.sum(
        jnp.where(own_slot == slots[0], wtt[pl.ds(0, 1), :], 0.0)
        + jnp.where(own_slot == slots[1], wtt[pl.ds(1, 1), :], 0.0),
        axis=1,
        keepdims=True,
    )
    row8 = iota((8, SEQS), 0)
    slot_cols = jnp.where(row8 == 0, slots[0], slots[1]).astype(F32).T.astype(jnp.int32)
    slot_lane = iota((SEQS, EXPERTS * CAPACITY), 1)
    place_t[...] = jnp.where(
        (slot_lane == slot_cols[:, 0:1]) | (slot_lane == slot_cols[:, 1:2]), 1.0, 0.0
    ).astype(BF16)

    arrived("graw", "lens", "fbias", "qgain", "kgain")
    for b in range(OWN):
        for h in range(2):
            gates[pl.ds(h * OWN + b, 1), :] = graw[b, pl.ds(h, 1), :]
    seq_row = lax.rem(iota((2 * OWN, OWN), 0), OWN)
    len_col = jnp.sum(
        jnp.where(seq_row == iota((2 * OWN, OWN), 1), lens[...].astype(F32), 0.0),
        axis=1,
        keepdims=True,
    ).astype(jnp.int32)
    position = iota((2 * OWN, 1024), 1)
    gate_rows = gates[...]
    latest = jnp.sum(jnp.where(position == len_col - 1, gate_rows, 0.0), axis=1, keepdims=True)
    gates[...] = jnp.where(position < len_col, -gate_rows, -jnp.inf)
    lane16 = iota((1, 16), 1)
    bias = [
        jnp.sum(jnp.where(lane16 == 2 * t + h, fbias[...], 0.0), axis=1, keepdims=True)
        for h in range(2)
    ]
    for copy in kv:
        copy.wait()

    landed(first)
    sums = send1[e].astype(F32)
    for j in range(1, EP):
        sums = sums + recv1[j].astype(F32)
    stat = sums[:, 512:640]
    stat = stat + pltpu.roll(stat, 64, 1)
    lane = iota((OWN, HEAD), 1)

    def stat_at(index):
        return jnp.sum(jnp.where(lane == index, stat, 0.0), axis=1, keepdims=True)

    scale = lax.rsqrt(stat_at(16) / D + EPS)
    forget = []
    for h in range(2):
        logit = stat_at(2 * t + h) * scale + bias[h]
        forget.append(jnp.minimum(logit, 0.0) - jnp.log(1.0 + jnp.exp(-jnp.abs(logit))))

    def head_norm(rows, gain):
        mean = jnp.mean(rows * rows, axis=1, keepdims=True)
        return (rows * lax.rsqrt(mean + EPS) * gain).astype(BF16)

    queries = jnp.concatenate(
        [head_norm(sums[:, h * HEAD : (h + 1) * HEAD], qgain[...]) for h in range(2)], axis=0
    ).astype(F32)
    new_key = head_norm(sums[:, 256:384], kgain[...])
    new_value = (sums[:, 384:512] * scale).astype(BF16)
    keys_out[...] = new_key
    values_out[...] = new_value
    twice_key = jnp.concatenate([new_key, new_key], axis=0).astype(F32)
    twice_value = jnp.concatenate([new_value, new_value], axis=0).astype(F32)
    now = latest + jnp.concatenate(forget, axis=0)
    self_score = jnp.sum(queries * twice_key, axis=1, keepdims=True) * FACTOR

    q_row = lax.rem(iota((2 * OWN, HEAD), 0), OWN)
    spread = jnp.concatenate(
        [jnp.where(q_row == b, queries, 0.0).astype(BF16) for b in range(OWN)], axis=1
    )
    scores = lax.dot_general(spread, kcat[...], NT, preferred_element_type=F32)
    scores = scores * FACTOR + now + gates[...]
    ceiling = jnp.maximum(jnp.max(scores, axis=1, keepdims=True), self_score)
    weights = jnp.exp(scores - ceiling)
    self_weight = jnp.exp(self_score - ceiling)
    denominator = jnp.sum(weights, axis=1, keepdims=True) + self_weight
    p_row = lax.rem(iota((2 * OWN, 1024), 0), OWN)
    out = self_weight * twice_value
    for b in range(OWN):
        out = out + mm(jnp.where(p_row == b, weights, 0.0).astype(BF16), vbuf[b])
    out = out / denominator
    heads[e] = jnp.concatenate([out[0:OWN], out[OWN : 2 * OWN]], axis=1).astype(BF16)

    second = to_ep(1, lambda peer: heads.at[e], lambda j: heads.at[e])
    arrived("wout", "fgain", "mixv", "dd", "g0", "g1", "u0", "u1", "d0", "d1")
    arrived(*[f"dg{c}" for c in range(CHUNKS)], *[f"du{c}" for c in range(CHUNKS)])
    landed(second)
    attn = mm(heads[...].reshape(SEQS, 256), wout[...])
    add_over_tp(0, attn, hid, halves, other, chips, mid)

    middle = mid[...]
    per_owner = middle.astype(F32).reshape(EP, OWN, HEAD)
    own_part = jnp.where(core == 0, per_owner[:, 0:8], per_owner[:, 8:16])
    picked = mm(place[...], middle).reshape(EP, CAPACITY, HEAD)
    send4[...] = jnp.concatenate([picked, own_part], axis=1).astype(BF16)
    rows = to_ep(2, lambda peer: send4.at[peer], lambda j: xrows.at[core, :, own_cols])
    normed_mid = (middle.astype(F32) * fgain[:, own_cols]).astype(BF16)
    dense = []
    for c in range(CHUNKS):
        dense_part = mm(normed_mid, wdense[:, 2 * c * WIDE : 2 * (c + 1) * WIDE])
        send4d[c] = dense_part.astype(BF16).reshape(EP, OWN, 2 * WIDE)
        dense.append(
            to_ep(5 + c, lambda peer: send4d.at[c, peer], lambda j: recv4d.at[c, j])
        )
    xrows[core, :, own_cols] = send4[e]
    landed(rows)
    shared = to_tp(sibling, xrows.at[core], xrows.at[core], 10)
    shared.wait_recv()
    tp_copies.append(shared)

    arrived_rows = [xrows[k].astype(F32) for k in range(2)]
    routed = jnp.concatenate([r[0:CAPACITY] for r in arrived_rows], axis=0)
    slot_scale = lax.rsqrt(jnp.sum(routed * routed, axis=1, keepdims=True) / D + EPS)
    routed_in = (routed * fgain[...]).astype(BF16)
    both_pre = mm(routed_in, wgu[...])
    upper = iota((48, HEAD), 0) < CAPACITY
    gate_pre = jnp.where(upper, both_pre[:, 0:128], both_pre[:, 128:256]) * slot_scale
    up_pre = jnp.where(upper, both_pre[:, 256:384], both_pre[:, 384:512]) * slot_scale
    unit = silu(gate_pre) * up_pre
    units = jnp.concatenate(
        [jnp.where(upper, unit, 0.0), jnp.where(upper, 0.0, unit)], axis=1
    ).astype(BF16)
    send5[...] = (mm(units, wdn[...]) * slot_weight).astype(BF16)
    back = to_ep(
        3,
        lambda peer: send5.at[:, pl.ds(pl.multiple_of(peer * HEAD, HEAD), HEAD)],
        lambda j: ret.at[e],
    )
    ret[e] = send5[:, own_cols]

    own_mid = jnp.concatenate([r[CAPACITY:] for r in arrived_rows], axis=0)
    mid_scale = lax.rsqrt(jnp.sum(own_mid * own_mid, axis=1, keepdims=True) / D + EPS)
    own_normed = (own_mid * fgain[...]).astype(BF16).astype(F32)
    mix_rows = mixv[...].astype(F32)
    mix_dot = sum(
        own_normed[:, s * HEAD : (s + 1) * HEAD] * mix_rows[s : s + 1] for s in range(EP)
    ).sum(axis=1, keepdims=True)
    share = jax.nn.sigmoid(mid_scale * mix_dot)
    hidden_copies = []
    for c in range(CHUNKS):
        landed(dense[c])
        dsums = send4d[c, e].astype(F32)
        for j in range(1, EP):
            dsums = dsums + recv4d[c, j].astype(F32)
        dense_unit = silu(dsums[:, :WIDE] * mid_scale) * (dsums[:, WIDE:] * mid_scale)
        dhid[c, e] = (dense_unit * share).astype(BF16)
        hidden_copies.append(
            to_ep(5 + CHUNKS + c, lambda peer: dhid.at[c, e], lambda j: dhid.at[c, e])
        )

    landed(back)
    branch = mm(place_t[...], ret[...].reshape(EXPERTS * CAPACITY, HEAD))
    for c in range(CHUNKS):
        landed(hidden_copies[c])
        branch = branch + mm(
            dhid[c].reshape(SEQS, WIDE), wdd[c * WIDE : (c + 1) * WIDE, :]
        )
    add_over_tp(1, branch, mid, halves2, other2, chips2, final)
    mixed_out[...] = final[...]
    groups = [first, second, rows, back, tp_copies]
    for copies in groups + dense + hidden_copies:
        for copy in copies:
            copy.wait_send()


def on_device(
    hidden_in, attn_gain, forget_weight, forget_bias, query_weight, key_weight, value_weight,
    query_gain, key_gain, cache_keys, cache_values, cache_gates, lengths, output_weight,
    ffn_gain, route_group, route_expert, route_weight, expert_gate, expert_up, expert_down,
    mix_vector, dense_gate, dense_up, dense_down,
):
    vmem = pltpu.VMEM
    anywhere = pl.BlockSpec(memory_space=pltpu.HBM)
    scratch = [
        vmem((SEQS, HEAD), BF16),
        vmem((1, D), F32),
        vmem((HEAD, HEAD), BF16),
        vmem((1, 16), F32),
        vmem((HEAD, 512), BF16),
        vmem((1, HEAD), F32),
        vmem((1, HEAD), F32),
        vmem((1024, OWN * HEAD), BF16),
        vmem((OWN, 1024, HEAD), BF16),
        vmem((OWN, 2, 1024), F32),
        vmem((1, OWN), jnp.int32),
        vmem((256, HEAD), BF16),
        vmem((1, D), F32),
        vmem((1, SEQS), jnp.int32),
        vmem((2, SEQS), jnp.int32),
        vmem((2, SEQS), F32),
        vmem((D, 512), BF16),
        vmem((256, D), BF16),
        vmem((16, HEAD), BF16),
        vmem((HEAD, 1024), BF16),
        vmem((512, HEAD), BF16),
        vmem((EP, OWN, 640), BF16),
        vmem((EP, OWN, 640), BF16),
        vmem((2 * OWN, 1024), F32),
        vmem((EP * CAPACITY, SEQS), BF16),
        vmem((SEQS, EXPERTS * CAPACITY), BF16),
        vmem((EP, OWN, 256), BF16),
        vmem((2, 128, HEAD), F32),
        vmem((128, HEAD), F32),
        vmem((4, 128, HEAD), BF16),
        vmem((SEQS, HEAD), BF16),
        vmem((EP, 32, HEAD), BF16),
        vmem((2, 32, D), BF16),
        vmem((CHUNKS, EP, OWN, 2 * WIDE), BF16),
        vmem((CHUNKS, EP, OWN, 2 * WIDE), BF16),
        vmem((48, D), BF16),
        vmem((EP, 48, HEAD), BF16),
        vmem((CHUNKS, EP, OWN, WIDE), BF16),
        vmem((2, 128, HEAD), F32),
        vmem((128, HEAD), F32),
        vmem((4, 128, HEAD), BF16),
        vmem((SEQS, HEAD), BF16),
        pltpu.SemaphoreType.DMA((24 + 2 * CHUNKS,)),
        pltpu.SemaphoreType.DMA((2, OWN)),
        pltpu.SemaphoreType.DMA((5 + 2 * CHUNKS, EP)),
        pltpu.SemaphoreType.DMA((5 + 2 * CHUNKS, EP)),
        pltpu.SemaphoreType.DMA((11,)),
        pltpu.SemaphoreType.DMA((11,)),
    ]
    call = pl.pallas_call(
        layer,
        out_shape=(
            vmem((SEQS, HEAD), BF16),
            vmem((OWN, HEAD), BF16),
            vmem((OWN, HEAD), BF16),
        ),
        in_specs=[anywhere] * 25,
        out_specs=(pl.BlockSpec(memory_space=pltpu.VMEM),) * 3,
        scratch_shapes=scratch,
        compiler_params=pltpu.CompilerParams(
            collective_id=0, has_side_effects=True, vmem_limit_bytes=60 * 1024 * 1024
        ),
    )
    results = call(
        hidden_in,
        attn_gain.reshape(1, D),
        forget_weight.T,
        forget_bias.reshape(1, 16),
        query_weight,
        key_weight,
        value_weight,
        query_gain.reshape(1, HEAD),
        key_gain.reshape(1, HEAD),
        cache_keys.reshape(OWN, 1024, HEAD),
        cache_values.reshape(OWN, 1024, HEAD),
        cache_gates,
        lengths.reshape(1, OWN),
        output_weight,
        ffn_gain.reshape(1, D),
        route_group.reshape(1, SEQS),
        route_expert.T,
        route_weight.T,
        expert_gate,
        expert_up,
        expert_down,
        mix_vector.reshape(16, HEAD),
        dense_gate,
        dense_up,
        dense_down,
    )
    return pl.pallas_call(
        put_out,
        out_shape=[jax.ShapeDtypeStruct(r.shape, r.dtype) for r in results],
        in_specs=[pl.BlockSpec(memory_space=pltpu.VMEM)] * 3,
        out_specs=[anywhere] * 3,
        scratch_shapes=[pltpu.SemaphoreType.DMA((3,))],
        compiler_params=pltpu.CompilerParams(vmem_limit_bytes=1024 * 1024),
    )(*results)


def solution(mesh):
    placed = (
        P(None, "ep"), P(), P(), P(), P("ep", "tp"), P("ep", "tp"), P("ep", "tp"), P(), P(),
        P("ep", "tp", None, None), P("ep", "tp", None, None), P("ep", "tp", None), P("ep"),
        P("tp", "ep"), P(), P(), P(), P(), P("ep", None, "tp"), P("ep", None, "tp"),
        P("ep", "tp", None), P(), P("ep", "tp"), P("ep", "tp"), P("tp", "ep"),
    )
    return jax.shard_map(
        on_device,
        mesh=mesh,
        in_specs=placed,
        out_specs=(P(None, "ep"), P("ep", "tp"), P("ep", "tp")),
        check_vma=False,
    )
```

```python
import jax
import jax.numpy as jnp
from jax import lax
from jax.experimental import pallas as pl
from jax.experimental.pallas import tpu as pltpu
from jax.sharding import PartitionSpec as P

D = 2048
HEAD = 128
GROUP_EXPERTS = 4
CAPACITY = 24
EXPERTS = 32
SEQS = 256
EP = 16
OWN = SEQS // EP
CHUNKS = 2
WIDE = 512 // CHUNKS
EPS = 1e-06
FACTOR = HEAD**-0.5
F32 = jnp.float32
BF16 = jnp.bfloat16
MESH_ID = pl.DeviceIdType.MESH
NT = (((1,), (1,)), ((), ()))

EP_OFFSETS = [(2, 2), (2, 1), (1, 2), (2, 3), (3, 2), (2, 0), (0, 2), (1, 1), (3, 3), (1, 3), (3, 1), (0, 1), (3, 0), (0, 3), (1, 0)]


def mm(a, b):
    return jnp.dot(a, b, preferred_element_type=F32)


def iota(shape, dim):
    return lax.broadcasted_iota(jnp.int32, shape, dim)


def silu(v):
    return v * jax.nn.sigmoid(v)


def put_out(mixed, keys, values, mixed_out, keys_out, values_out, sems):
    copies = [
        pltpu.make_async_copy(src, dst, sems.at[i])
        for i, (src, dst) in enumerate(
            ((mixed, mixed_out), (keys, keys_out), (values, values_out))
        )
    ]
    for copy in copies:
        copy.start()
    for copy in copies:
        copy.wait()


def layer(
    hidden, attn_gain, forget_t, forget_bias, query_w, key_w, value_w, query_gain, key_gain,
    cache_k, cache_v, cache_g, lengths, output_w, ffn_gain, group, expert_t, weight_t,
    gate_w, up_w, down_w, mix_vector, dense_gate, dense_up, dense_down,
    mixed_out, keys_out, values_out,
    hid, again, fwt, fbias, wqkv, qgain, kgain, kcat, vbuf, graw, lens, wout, fgain,
    grp, ext, wtt, wgu, wdn, mixv, wdense, wdd,
    send1, recv1, gates, place, place_t, heads, halves, other, chips, mid,
    send4, xrows, send4d, recv4d, send5, ret, dhid, halves2, other2, chips2, final,
    load_sem, kv_sem, ep_send, ep_recv, tp_send, tp_recv,
):
    e = lax.axis_index("ep")
    t = lax.axis_index("tp")
    z = lax.div(e, 4)
    x = lax.rem(e, 4)
    ep_peers = [
        (dz * 4 + dx, lax.rem(z + dz, 4) * 4 + lax.rem(x + dx, 4)) for dz, dx in EP_OFFSETS
    ]
    y = lax.div(t, 2)
    core = lax.rem(t, 2)
    sibling = t + 1 - 2 * core
    y_peers = [(j, lax.rem(y + j, 4) * 2 + core) for j in (2, 1, 3)]
    own_cols = pl.ds(pl.multiple_of(e * HEAD, HEAD), HEAD)

    barrier = pltpu.get_barrier_semaphore()
    for _, peer in ep_peers:
        pl.semaphore_signal(barrier, inc=1, device_id={"ep": peer}, device_id_type=MESH_ID)
    for peer in [peer for _, peer in y_peers] + [sibling]:
        pl.semaphore_signal(barrier, inc=1, device_id={"tp": peer}, device_id_type=MESH_ID)

    loads = {}

    def load(name, src, dst):
        copy = pltpu.make_async_copy(src, dst, load_sem.at[len(loads)])
        copy.start()
        loads[name] = copy

    load("hid", hidden, hid)
    load("again", attn_gain, again)
    load("fwt", forget_t.at[:, own_cols], fwt.at[pl.ds(0, 16)])
    load("wq", query_w, wqkv.at[:, pl.ds(0, 256)])
    load("wk", key_w, wqkv.at[:, pl.ds(256, 128)])
    load("wv", value_w, wqkv.at[:, pl.ds(384, 128)])
    load("grp", group, grp)
    load("ext", expert_t, ext)
    load("wtt", weight_t, wtt)
    load("graw", cache_g, graw)
    load("lens", lengths, lens)
    load("fbias", forget_bias, fbias)
    load("qgain", query_gain, qgain)
    load("kgain", key_gain, kgain)
    kv = []
    for b in range(OWN):
        copy = pltpu.make_async_copy(
            cache_k.at[b], kcat.at[:, pl.ds(b * HEAD, HEAD)], kv_sem.at[0, b]
        )
        copy.start()
        kv.append(copy)
    for b in range(OWN):
        copy = pltpu.make_async_copy(cache_v.at[b], vbuf.at[b], kv_sem.at[1, b])
        copy.start()
        kv.append(copy)
    load("wout", output_w, wout)
    load("fgain", ffn_gain, fgain)
    load("mixv", mix_vector, mixv)
    for c in range(CHUNKS):
        cols = pl.ds(c * WIDE, WIDE)
        load(f"dg{c}", dense_gate.at[:, cols], wdense.at[:, pl.ds(2 * c * WIDE, WIDE)])
        load(f"du{c}", dense_up.at[:, cols], wdense.at[:, pl.ds((2 * c + 1) * WIDE, WIDE)])
    load("dd", dense_down, wdd)
    for i in range(2):
        load(f"g{i}", gate_w.at[i], wgu.at[:, pl.ds(i * 128, 128)])
        load(f"u{i}", up_w.at[i], wgu.at[:, pl.ds(256 + i * 128, 128)])
        load(f"d{i}", down_w.at[i], wdn.at[pl.ds(i * 128, 128)])

    def arrived(*names):
        for name in names:
            loads[name].wait()

    def to_ep(stage, src_of, dst_of):
        copies = []
        for j, peer in ep_peers:
            copy = pltpu.make_async_remote_copy(
                src_ref=src_of(peer),
                dst_ref=dst_of(j),
                send_sem=ep_send.at[stage, j],
                recv_sem=ep_recv.at[stage, j],
                device_id={"ep": peer},
                device_id_type=MESH_ID,
            )
            copy.start()
            copies.append(copy)
        return copies

    def to_tp(peer, src, dst, index):
        copy = pltpu.make_async_remote_copy(
            src_ref=src,
            dst_ref=dst,
            send_sem=tp_send.at[index],
            recv_sem=tp_recv.at[index],
            device_id={"tp": peer},
            device_id_type=MESH_ID,
        )
        copy.start()
        return copy

    def landed(copies):
        for copy in copies:
            copy.wait_recv()

    half = pl.ds(pl.multiple_of(core * 128, 128), 128)
    tp_copies = []

    def add_over_tp(stage, terms, base, halves, other, chips, dst):
        halves[...] = terms.reshape(2, 128, HEAD)
        pair = to_tp(sibling, halves.at[1 - core], other, 5 * stage)
        pair.wait_recv()
        chips[y] = (halves[core] + other[...]).astype(BF16)
        along = [
            to_tp(peer, chips.at[y], chips.at[y], 5 * stage + j) for j, peer in y_peers
        ]
        landed(along)
        total = base[half, :].astype(F32)
        for chip in range(4):
            total = total + chips[chip].astype(F32)
        dst[half, :] = total.astype(BF16)
        last = to_tp(sibling, dst.at[half], dst.at[half], 5 * stage + 4)
        last.wait_recv()
        tp_copies.extend([pair, last, *along])

    fwt[pl.ds(16, 112), :] = jnp.zeros((112, HEAD), BF16)
    arrived("hid", "again", "fwt", "wq", "wk", "wv")
    stream = hid[...].astype(F32)
    normed = (stream * again[:, own_cols]).astype(BF16)
    projected = mm(normed, wqkv[...]).astype(BF16)
    send1[:, :, 0:512] = projected.reshape(EP, OWN, 512)
    stats = lax.dot_general(normed, fwt[...], NT, preferred_element_type=F32)
    lane = iota((SEQS, HEAD), 1)
    stats = jnp.where(lane == 16, jnp.sum(stream * stream, axis=1, keepdims=True), stats)
    high = stats.astype(BF16).astype(F32)
    low = stats - high
    both = jnp.where(lane < 64, high, pltpu.roll(low, 64, 1)).astype(BF16)
    send1[:, :, 512:640] = both.reshape(EP, OWN, HEAD)
    pl.semaphore_wait(barrier, EP - 1 + 4)
    sent = to_ep(0, lambda peer: send1.at[peer], lambda j: recv1.at[j])
    first = sent

    arrived("grp", "ext", "wtt")
    chosen = [grp[...] * GROUP_EXPERTS + ext[pl.ds(k, 1), :] for k in range(2)]
    expert_row = iota((EXPERTS, SEQS), 0)
    hits = [jnp.where(expert_row == chosen[k], 1.0, 0.0) for k in range(2)]
    any_hit = hits[0] + hits[1]
    before = jnp.where(iota((SEQS, SEQS), 0) < iota((SEQS, SEQS), 1), 1.0, 0.0).astype(BF16)
    rank = mm(any_hit.astype(BF16), before)
    slot_of = rank + (expert_row * CAPACITY).astype(F32)
    slots = [
        jnp.sum(hits[k] * slot_of, axis=0, keepdims=True).astype(jnp.int32) for k in range(2)
    ]
    three = (EP, CAPACITY, SEQS)
    slot_row = (2 * iota(three, 0) + core) * CAPACITY + iota(three, 1)
    hit = (slot_row == slots[0][None]) | (slot_row == slots[1][None])
    place[...] = jnp.where(hit, 1.0, 0.0).reshape(EP * CAPACITY, SEQS).astype(BF16)
    own_slot = iota((48, SEQS), 0) + e * 48
    slot_weight = jnp.sum(
        jnp.where(own_slot == slots[0], wtt[pl.ds(0, 1), :], 0.0)
        + jnp.where(own_slot == slots[1], wtt[pl.ds(1, 1), :], 0.0),
        axis=1,
        keepdims=True,
    )
    row8 = iota((8, SEQS), 0)
    slot_cols = jnp.where(row8 == 0, slots[0], slots[1]).astype(F32).T.astype(jnp.int32)
    slot_lane = iota((SEQS, EXPERTS * CAPACITY), 1)
    place_t[...] = jnp.where(
        (slot_lane == slot_cols[:, 0:1]) | (slot_lane == slot_cols[:, 1:2]), 1.0, 0.0
    ).astype(BF16)

    arrived("graw", "lens", "fbias", "qgain", "kgain")
    for b in range(OWN):
        for h in range(2):
            gates[pl.ds(h * OWN + b, 1), :] = graw[b, pl.ds(h, 1), :]
    seq_row = lax.rem(iota((2 * OWN, OWN), 0), OWN)
    len_col = jnp.sum(
        jnp.where(seq_row == iota((2 * OWN, OWN), 1), lens[...].astype(F32), 0.0),
        axis=1,
        keepdims=True,
    ).astype(jnp.int32)
    position = iota((2 * OWN, 1024), 1)
    gate_rows = gates[...]
    latest = jnp.sum(jnp.where(position == len_col - 1, gate_rows, 0.0), axis=1, keepdims=True)
    gates[...] = jnp.where(position < len_col, -gate_rows, -jnp.inf)
    lane16 = iota((1, 16), 1)
    bias = [
        jnp.sum(jnp.where(lane16 == 2 * t + h, fbias[...], 0.0), axis=1, keepdims=True)
        for h in range(2)
    ]
    for copy in kv:
        copy.wait()

    landed(first)
    sums = send1[e].astype(F32)
    for j in range(1, EP):
        sums = sums + recv1[j].astype(F32)
    stat = sums[:, 512:640]
    stat = stat + pltpu.roll(stat, 64, 1)
    lane = iota((OWN, HEAD), 1)

    def stat_at(index):
        return jnp.sum(jnp.where(lane == index, stat, 0.0), axis=1, keepdims=True)

    scale = lax.rsqrt(stat_at(16) / D + EPS)
    forget = []
    for h in range(2):
        logit = stat_at(2 * t + h) * scale + bias[h]
        forget.append(jnp.minimum(logit, 0.0) - jnp.log(1.0 + jnp.exp(-jnp.abs(logit))))

    def head_norm(rows, gain):
        mean = jnp.mean(rows * rows, axis=1, keepdims=True)
        return (rows * lax.rsqrt(mean + EPS) * gain).astype(BF16)

    queries = jnp.concatenate(
        [head_norm(sums[:, h * HEAD : (h + 1) * HEAD], qgain[...]) for h in range(2)], axis=0
    ).astype(F32)
    new_key = head_norm(sums[:, 256:384], kgain[...])
    new_value = (sums[:, 384:512] * scale).astype(BF16)
    keys_out[...] = new_key
    values_out[...] = new_value
    twice_key = jnp.concatenate([new_key, new_key], axis=0).astype(F32)
    twice_value = jnp.concatenate([new_value, new_value], axis=0).astype(F32)
    now = latest + jnp.concatenate(forget, axis=0)
    self_score = jnp.sum(queries * twice_key, axis=1, keepdims=True) * FACTOR

    q_row = lax.rem(iota((2 * OWN, HEAD), 0), OWN)
    spread = jnp.concatenate(
        [jnp.where(q_row == b, queries, 0.0).astype(BF16) for b in range(OWN)], axis=1
    )
    scores = lax.dot_general(spread, kcat[...], NT, preferred_element_type=F32)
    scores = scores * FACTOR + now + gates[...]
    ceiling = jnp.maximum(jnp.max(scores, axis=1, keepdims=True), self_score)
    weights = jnp.exp(scores - ceiling)
    self_weight = jnp.exp(self_score - ceiling)
    denominator = jnp.sum(weights, axis=1, keepdims=True) + self_weight
    p_row = lax.rem(iota((2 * OWN, 1024), 0), OWN)
    out = self_weight * twice_value
    for b in range(OWN):
        out = out + mm(jnp.where(p_row == b, weights, 0.0).astype(BF16), vbuf[b])
    out = out / denominator
    heads[e] = jnp.concatenate([out[0:OWN], out[OWN : 2 * OWN]], axis=1).astype(BF16)

    second = to_ep(1, lambda peer: heads.at[e], lambda j: heads.at[e])
    arrived("wout", "fgain", "mixv", "dd", "g0", "g1", "u0", "u1", "d0", "d1")
    arrived(*[f"dg{c}" for c in range(CHUNKS)], *[f"du{c}" for c in range(CHUNKS)])
    landed(second)
    attn = mm(heads[...].reshape(SEQS, 256), wout[...])
    add_over_tp(0, attn, hid, halves, other, chips, mid)

    middle = mid[...]
    per_owner = middle.astype(F32).reshape(EP, OWN, HEAD)
    own_part = jnp.where(core == 0, per_owner[:, 0:8], per_owner[:, 8:16])
    picked = mm(place[...], middle).reshape(EP, CAPACITY, HEAD)
    send4[...] = jnp.concatenate([picked, own_part], axis=1).astype(BF16)
    rows = to_ep(2, lambda peer: send4.at[peer], lambda j: xrows.at[core, :, own_cols])
    normed_mid = (middle.astype(F32) * fgain[:, own_cols]).astype(BF16)
    dense = []
    for c in range(CHUNKS):
        dense_part = mm(normed_mid, wdense[:, 2 * c * WIDE : 2 * (c + 1) * WIDE])
        send4d[c] = dense_part.astype(BF16).reshape(EP, OWN, 2 * WIDE)
        dense.append(
            to_ep(5 + c, lambda peer: send4d.at[c, peer], lambda j: recv4d.at[c, j])
        )
    xrows[core, :, own_cols] = send4[e]
    landed(rows)
    shared = to_tp(sibling, xrows.at[core], xrows.at[core], 10)
    shared.wait_recv()
    tp_copies.append(shared)

    arrived_rows = [xrows[k].astype(F32) for k in range(2)]
    routed = jnp.concatenate([r[0:CAPACITY] for r in arrived_rows], axis=0)
    slot_scale = lax.rsqrt(jnp.sum(routed * routed, axis=1, keepdims=True) / D + EPS)
    routed_in = (routed * fgain[...]).astype(BF16)
    both_pre = mm(routed_in, wgu[...])
    upper = iota((48, HEAD), 0) < CAPACITY
    gate_pre = jnp.where(upper, both_pre[:, 0:128], both_pre[:, 128:256]) * slot_scale
    up_pre = jnp.where(upper, both_pre[:, 256:384], both_pre[:, 384:512]) * slot_scale
    unit = silu(gate_pre) * up_pre
    units = jnp.concatenate(
        [jnp.where(upper, unit, 0.0), jnp.where(upper, 0.0, unit)], axis=1
    ).astype(BF16)
    send5[...] = (mm(units, wdn[...]) * slot_weight).astype(BF16)
    back = to_ep(
        3,
        lambda peer: send5.at[:, pl.ds(pl.multiple_of(peer * HEAD, HEAD), HEAD)],
        lambda j: ret.at[e],
    )
    ret[e] = send5[:, own_cols]

    own_mid = jnp.concatenate([r[CAPACITY:] for r in arrived_rows], axis=0)
    mid_scale = lax.rsqrt(jnp.sum(own_mid * own_mid, axis=1, keepdims=True) / D + EPS)
    own_normed = (own_mid * fgain[...]).astype(BF16).astype(F32)
    mix_rows = mixv[...].astype(F32)
    mix_dot = sum(
        own_normed[:, s * HEAD : (s + 1) * HEAD] * mix_rows[s : s + 1] for s in range(EP)
    ).sum(axis=1, keepdims=True)
    share = jax.nn.sigmoid(mid_scale * mix_dot)
    hidden_copies = []
    for c in range(CHUNKS):
        landed(dense[c])
        dsums = send4d[c, e].astype(F32)
        for j in range(1, EP):
            dsums = dsums + recv4d[c, j].astype(F32)
        dense_unit = silu(dsums[:, :WIDE] * mid_scale) * (dsums[:, WIDE:] * mid_scale)
        dhid[c, e] = (dense_unit * share).astype(BF16)
        hidden_copies.append(
            to_ep(5 + CHUNKS + c, lambda peer: dhid.at[c, e], lambda j: dhid.at[c, e])
        )

    landed(back)
    branch = mm(place_t[...], ret[...].reshape(EXPERTS * CAPACITY, HEAD))
    for c in range(CHUNKS):
        landed(hidden_copies[c])
        branch = branch + mm(
            dhid[c].reshape(SEQS, WIDE), wdd[c * WIDE : (c + 1) * WIDE, :]
        )
    add_over_tp(1, branch, mid, halves2, other2, chips2, final)
    mixed_out[...] = final[...]
    groups = [first, second, rows, back, tp_copies]
    for copies in groups + dense + hidden_copies:
        for copy in copies:
            copy.wait_send()


def on_device(
    hidden_in, attn_gain, forget_weight, forget_bias, query_weight, key_weight, value_weight,
    query_gain, key_gain, cache_keys, cache_values, cache_gates, lengths, output_weight,
    ffn_gain, route_group, route_expert, route_weight, expert_gate, expert_up, expert_down,
    mix_vector, dense_gate, dense_up, dense_down,
):
    vmem = pltpu.VMEM
    anywhere = pl.BlockSpec(memory_space=pltpu.HBM)
    scratch = [
        vmem((SEQS, HEAD), BF16),
        vmem((1, D), F32),
        vmem((HEAD, HEAD), BF16),
        vmem((1, 16), F32),
        vmem((HEAD, 512), BF16),
        vmem((1, HEAD), F32),
        vmem((1, HEAD), F32),
        vmem((1024, OWN * HEAD), BF16),
        vmem((OWN, 1024, HEAD), BF16),
        vmem((OWN, 2, 1024), F32),
        vmem((1, OWN), jnp.int32),
        vmem((256, HEAD), BF16),
        vmem((1, D), F32),
        vmem((1, SEQS), jnp.int32),
        vmem((2, SEQS), jnp.int32),
        vmem((2, SEQS), F32),
        vmem((D, 512), BF16),
        vmem((256, D), BF16),
        vmem((16, HEAD), BF16),
        vmem((HEAD, 1024), BF16),
        vmem((512, HEAD), BF16),
        vmem((EP, OWN, 640), BF16),
        vmem((EP, OWN, 640), BF16),
        vmem((2 * OWN, 1024), F32),
        vmem((EP * CAPACITY, SEQS), BF16),
        vmem((SEQS, EXPERTS * CAPACITY), BF16),
        vmem((EP, OWN, 256), BF16),
        vmem((2, 128, HEAD), F32),
        vmem((128, HEAD), F32),
        vmem((4, 128, HEAD), BF16),
        vmem((SEQS, HEAD), BF16),
        vmem((EP, 32, HEAD), BF16),
        vmem((2, 32, D), BF16),
        vmem((CHUNKS, EP, OWN, 2 * WIDE), BF16),
        vmem((CHUNKS, EP, OWN, 2 * WIDE), BF16),
        vmem((48, D), BF16),
        vmem((EP, 48, HEAD), BF16),
        vmem((CHUNKS, EP, OWN, WIDE), BF16),
        vmem((2, 128, HEAD), F32),
        vmem((128, HEAD), F32),
        vmem((4, 128, HEAD), BF16),
        vmem((SEQS, HEAD), BF16),
        pltpu.SemaphoreType.DMA((24 + 2 * CHUNKS,)),
        pltpu.SemaphoreType.DMA((2, OWN)),
        pltpu.SemaphoreType.DMA((5 + 2 * CHUNKS, EP)),
        pltpu.SemaphoreType.DMA((5 + 2 * CHUNKS, EP)),
        pltpu.SemaphoreType.DMA((11,)),
        pltpu.SemaphoreType.DMA((11,)),
    ]
    call = pl.pallas_call(
        layer,
        out_shape=(
            vmem((SEQS, HEAD), BF16),
            vmem((OWN, HEAD), BF16),
            vmem((OWN, HEAD), BF16),
        ),
        in_specs=[anywhere] * 25,
        out_specs=(pl.BlockSpec(memory_space=pltpu.VMEM),) * 3,
        scratch_shapes=scratch,
        compiler_params=pltpu.CompilerParams(
            collective_id=0, has_side_effects=True, vmem_limit_bytes=60 * 1024 * 1024
        ),
    )
    results = call(
        hidden_in,
        attn_gain.reshape(1, D),
        forget_weight.T,
        forget_bias.reshape(1, 16),
        query_weight,
        key_weight,
        value_weight,
        query_gain.reshape(1, HEAD),
        key_gain.reshape(1, HEAD),
        cache_keys.reshape(OWN, 1024, HEAD),
        cache_values.reshape(OWN, 1024, HEAD),
        cache_gates,
        lengths.reshape(1, OWN),
        output_weight,
        ffn_gain.reshape(1, D),
        route_group.reshape(1, SEQS),
        route_expert.T,
        route_weight.T,
        expert_gate,
        expert_up,
        expert_down,
        mix_vector.reshape(16, HEAD),
        dense_gate,
        dense_up,
        dense_down,
    )
    return pl.pallas_call(
        put_out,
        out_shape=[jax.ShapeDtypeStruct(r.shape, r.dtype) for r in results],
        in_specs=[pl.BlockSpec(memory_space=pltpu.VMEM)] * 3,
        out_specs=[anywhere] * 3,
        scratch_shapes=[pltpu.SemaphoreType.DMA((3,))],
        compiler_params=pltpu.CompilerParams(vmem_limit_bytes=1024 * 1024),
    )(*results)


def solution(mesh):
    placed = (
        P(None, "ep"), P(), P(), P(), P("ep", "tp"), P("ep", "tp"), P("ep", "tp"), P(), P(),
        P("ep", "tp", None, None), P("ep", "tp", None, None), P("ep", "tp", None), P("ep"),
        P("tp", "ep"), P(), P(), P(), P(), P("ep", None, "tp"), P("ep", None, "tp"),
        P("ep", "tp", None), P(), P("ep", "tp"), P("ep", "tp"), P("tp", "ep"),
    )
    return jax.shard_map(
        on_device,
        mesh=mesh,
        in_specs=placed,
        out_specs=(P(None, "ep"), P("ep", "tp"), P("ep", "tp")),
        check_vma=False,
    )
```
